32 devices in a mesh: sp: 8 (over z, y), tp: 4 (over x, core).
Axes of the slice: x: 2, y: 2, z: 4, core: 2. Of those that a mesh axis runs over, the one named last changes fastest.
Arguments:
- residual: bfloat16 [8192, 2048], P('sp'), may hold values from -8 to 8
- query_wide: bfloat16 [8192, 1024], P('sp', 'tp'), may hold values from -6 to 6
- key_wide: bfloat16 [8192, 1024], P('sp', 'tp'), may hold values from -6 to 6
- value_wide: bfloat16 [8192, 2048], P('sp', 'tp'), may hold values from -6 to 6
- decay_wide: bfloat16 [8192, 1024], P('sp', 'tp'), may hold values from -12 to 12
- gate_wide: bfloat16 [8192, 2048], P('sp', 'tp'), may hold values from -6 to 6
- query_narrow: bfloat16 [8192, 512], P('sp', 'tp'), may hold values from -6 to 6
- key_narrow: bfloat16 [8192, 512], P('sp', 'tp'), may hold values from -6 to 6
- value_narrow: bfloat16 [8192, 2048], P('sp', 'tp'), may hold values from -6 to 6
- decay_narrow: bfloat16 [8192, 512], P('sp', 'tp'), may hold values from -12 to 12
- gate_narrow: bfloat16 [8192, 2048], P('sp', 'tp'), may hold values from -6 to 6
- head_gain: float32 [512], replicated, may hold values from 0.1 to 1.9
- out_wide: bfloat16 [2048, 2048], P('tp'), may hold values from -0.125 to 0.125
- out_narrow: bfloat16 [2048, 2048], P('tp'), may hold values from -0.125 to 0.125
- mlp_gain: float32 [2048], replicated, may hold values from 0.1 to 1.9
- up_weight: bfloat16 [2048, 4096], P('sp', 'tp'), may hold values from -0.125 to 0.125
- down_weight: bfloat16 [4096, 2048], P('tp', 'sp'), may hold values from -0.09375 to 0.09375
Outputs:
- layer_out: bfloat16 [8192, 2048], P('sp', 'tp')
The draws below stay inside these ranges and needn't reach their ends.
All inputs are finite; a program needn't handle non-finite values.
Results may differ from the reference program's by a relative error of at most 0.017.
Values may be sent and summed in bfloat16 or wider, within the bound.
A program may use at most 128 MiB of HBM per device.

```python
import math
import jax
import jax.numpy as jnp
from jax import lax

D = 2048
FF = 4096
HEADS = 4
HEAD_KA = 256
HEAD_KB = 128
HEAD_V = 512
BLOCK = 64
TOK_DEV = 1024
SEQUENCE_TOKENS = 8192
N_TP = 4


def draw_residual(key, part):
    column = jnp.arange(D, dtype=jnp.float32) / D
    baseline = jax.random.normal(jax.random.fold_in(key, 3), (SEQUENCE_TOKENS, D), jnp.float32)
    scale = 0.5 * jnp.power(4.0, column)
    return jnp.clip(baseline * scale[None, :], -8.0, 8.0).astype(jnp.bfloat16)


def decay_draw(key, head_width, salt):
    random_subkeys = jax.random.split(jax.random.fold_in(key, salt), 6)
    channel_count = HEADS * head_width
    ranking = jax.random.permutation(random_subkeys[0], HEADS)
    slow_heads = ranking < HEADS // 2
    jitter = jnp.clip(jax.random.normal(random_subkeys[1], (SEQUENCE_TOKENS, channel_count), jnp.float32), -3.0, 3.0)
    offsets = jax.random.uniform(random_subkeys[2], (SEQUENCE_TOKENS // TOK_DEV,), jnp.float32, -0.7, 0.7)
    slow_cols = jnp.repeat(slow_heads, head_width, total_repeat_length=channel_count)
    baseline = jnp.where(slow_cols, math.log(SEQUENCE_TOKENS / 4.0), 1.0)
    spread = jax.random.uniform(random_subkeys[3], (channel_count,), jnp.float32, -0.5, 0.5)
    grouped_rows = jax.random.randint(random_subkeys[4], (3,), 0, SEQUENCE_TOKENS)
    group_match = jnp.any(jnp.arange(SEQUENCE_TOKENS)[:, None] == grouped_rows[None, :], axis=1)
    group_depth = jax.random.uniform(random_subkeys[5], (SEQUENCE_TOKENS, 1), jnp.float32, 3.5, 8.0)
    row_offsets = jnp.repeat(offsets, TOK_DEV, total_repeat_length=SEQUENCE_TOKENS)
    before_activation = baseline[None, :] + spread[None, :] + row_offsets[:, None] + jitter
    before_activation = jnp.where(group_match[:, None], -group_depth, before_activation)
    return jnp.clip(before_activation, -12.0, 12.0).astype(jnp.bfloat16)


def draw_decay_wide(key, part):
    return decay_draw(key, HEAD_KA, 11)


def draw_decay_narrow(key, part):
    return decay_draw(key, HEAD_KB, 13)


def levels(rng, extent, pieces, least, largest):
    def one(dim, blocks):
        draws = jax.random.uniform(jax.random.fold_in(jax.random.fold_in(rng, 6), dim), (blocks,), jnp.float32, least / len(pieces), largest / len(pieces))
        return jnp.repeat(jnp.exp(draws), extent[dim] // blocks).reshape((-1,) + (1,) * (len(extent) - dim - 1))

    factor_of = one(*pieces[0])
    for cut in pieces[1:]:
        factor_of = factor_of * one(*cut)
    return factor_of


def centred(own_key, extent, scale, bound, pieces=(), kind=jnp.bfloat16):
    gain = levels(own_key, extent, pieces, -0.22, 0.18) if pieces else 1.0
    drawn = jax.random.normal(own_key, extent, jnp.float32) * scale * gain
    return jnp.minimum(jnp.maximum(drawn, -bound), bound).astype(kind)


def setup_inputs(seed: int = 0) -> dict:
    streams_of = jax.random.split(jax.random.key(seed), 18)
    residual = draw_residual(jax.random.fold_in(streams_of[17], 71), 0)
    query_wide = centred(streams_of[1], (SEQUENCE_TOKENS, HEADS * HEAD_KA), 1.0, 6.0, ((0, 8), (1, 4)))
    key_wide = centred(streams_of[2], (SEQUENCE_TOKENS, HEADS * HEAD_KA), 1.0, 6.0, ((0, 8), (1, 4)))
    value_wide = centred(streams_of[3], (SEQUENCE_TOKENS, HEADS * HEAD_V), 1.0, 6.0, ((0, 8), (1, 4)))
    decay_wide = draw_decay_wide(jax.random.fold_in(streams_of[17], 71), 0)
    gate_wide = centred(streams_of[5], (SEQUENCE_TOKENS, HEADS * HEAD_V), 1.0, 6.0, ((0, 8), (1, 4)))
    query_narrow = centred(streams_of[6], (SEQUENCE_TOKENS, HEADS * HEAD_KB), 1.0, 6.0, ((0, 8), (1, 4)))
    key_narrow = centred(streams_of[7], (SEQUENCE_TOKENS, HEADS * HEAD_KB), 1.0, 6.0, ((0, 8), (1, 4)))
    value_narrow = centred(streams_of[8], (SEQUENCE_TOKENS, HEADS * HEAD_V), 1.0, 6.0, ((0, 8), (1, 4)))
    decay_narrow = draw_decay_narrow(jax.random.fold_in(streams_of[17], 71), 0)
    gate_narrow = centred(streams_of[10], (SEQUENCE_TOKENS, HEADS * HEAD_V), 1.0, 6.0, ((0, 8), (1, 4)))
    head_gain = jnp.clip(1.0 + 0.18 * jax.random.normal(streams_of[11], (HEAD_V,), jnp.float32), 0.1, 1.9)
    out_wide = centred(streams_of[12], (HEADS * HEAD_V, D), (HEADS * HEAD_V) ** -0.5, 0.125, ((0, 4),))
    out_narrow = centred(streams_of[13], (HEADS * HEAD_V, D), (HEADS * HEAD_V) ** -0.5, 0.125, ((0, 4),))
    mlp_gain = jnp.clip(1.0 + 0.18 * jax.random.normal(streams_of[14], (D,), jnp.float32), 0.1, 1.9)
    up_weight = centred(streams_of[15], (D, FF), D ** -0.5, 0.125, ((0, 8), (1, 4)))
    down_weight = centred(streams_of[16], (FF, D), FF ** -0.5, 0.09375, ((0, 4), (1, 8)))
    return dict(residual=residual, query_wide=query_wide, key_wide=key_wide, value_wide=value_wide, decay_wide=decay_wide, gate_wide=gate_wide, query_narrow=query_narrow, key_narrow=key_narrow, value_narrow=value_narrow, decay_narrow=decay_narrow, gate_narrow=gate_narrow, head_gain=head_gain, out_wide=out_wide, out_narrow=out_narrow, mlp_gain=mlp_gain, up_weight=up_weight, down_weight=down_weight)


EPS = 1e-05
DECAY_NORMALIZER = 16.0
HIGHEST = lax.Precision.HIGHEST

def block_pass(queries, keys_in, values_in, log_decay, block_len):
    num_blocks = queries.shape[0] // block_len

    def to_blocks(stacked):
        return stacked.reshape((num_blocks, block_len) + stacked.shape[1:])
    causal = jnp.tril(jnp.ones((block_len, block_len), dtype=bool))
    initial = (jnp.zeros((queries.shape[1], queries.shape[2], values_in.shape[2]), jnp.float32), jnp.zeros((queries.shape[1], queries.shape[2]), jnp.float32))

    def advance(running, inputs):
        memory, offset = running
        block_q, block_k, block_v, block_g = inputs
        within = jnp.cumsum(block_g, axis=0)
        final_log = within[-1]
        scaled_q = block_q * jnp.exp(within)
        scaled_k = block_k * jnp.exp(-within)
        outside = jnp.einsum('ihd,hde->ihe', scaled_q, memory, precision=HIGHEST)
        scores = jnp.einsum('ihd,jhd->hij', scaled_q, scaled_k, precision=HIGHEST)
        scores = jnp.where(causal[None], scores, 0.0)
        inside = jnp.einsum('hij,jhe->ihe', scores, block_v, precision=HIGHEST)
        decayed_keys = scaled_k * jnp.exp(final_log)[None]
        memory = jnp.exp(final_log)[..., None] * memory + jnp.einsum('jhd,jhe->hde', decayed_keys, block_v, precision=HIGHEST)
        carried_q = scaled_q * jnp.exp(offset)[None]
        return ((memory, offset + final_log), (outside + inside, carried_q))
    (memory, totals), (outputs, carried_q) = lax.scan(advance, initial, (to_blocks(queries), to_blocks(keys_in), to_blocks(values_in), to_blocks(log_decay)))
    return (outputs.reshape(values_in.shape), carried_q.reshape(queries.shape), totals, memory)

def prepare(query, key_proj, value, decay, heads_here):
    row_count = query.shape[0]
    key_width = query.shape[1] // heads_here
    queries = query.astype(jnp.float32).reshape(row_count, heads_here, key_width) * key_width ** (-0.5)
    keys_in = key_proj.astype(jnp.float32).reshape(row_count, heads_here, key_width)
    values_in = value.astype(jnp.float32).reshape(row_count, heads_here, value.shape[1] // heads_here)
    log_decay = jax.nn.log_sigmoid(decay.astype(jnp.float32)).reshape(row_count, heads_here, key_width) / DECAY_NORMALIZER
    return (queries, keys_in, values_in, log_decay)

def finish(outputs, gate, head_gain):
    scale = lax.rsqrt(lax.optimization_barrier(jnp.mean(jnp.square(outputs), axis=-1, keepdims=True)) + EPS)
    gated = outputs * scale * head_gain * jax.nn.silu(gate.astype(jnp.float32).reshape(outputs.shape))
    return gated.reshape(outputs.shape[0], -1).astype(jnp.bfloat16)

def group_output(query, key_proj, value, decay, gate, head_gain):
    queries, keys_in, values_in, log_decay = prepare(query, key_proj, value, decay, HEADS)
    outputs = block_pass(queries, keys_in, values_in, log_decay, BLOCK)[0]
    return finish(outputs, gate, head_gain)

def blockwise_sum(left_sides, right_sides):
    total = jnp.zeros((left_sides[0].shape[0], right_sides[0].shape[1]), jnp.float32)
    for tp_block in range(N_TP):
        block_sum = jnp.zeros_like(total)
        for left_side, right_side in zip(left_sides, right_sides):
            block_width = left_side.shape[1] // N_TP
            first_col = tp_block * block_width
            block_sum = block_sum + jnp.dot(left_side[:, first_col:first_col + block_width], right_side[first_col:first_col + block_width], preferred_element_type=jnp.float32)
        total = total + lax.optimization_barrier(block_sum.astype(jnp.bfloat16)).astype(jnp.float32)
    return total

def reference(residual, query_wide, key_wide, value_wide, decay_wide, gate_wide, query_narrow, key_narrow, value_narrow, decay_narrow, gate_narrow, head_gain, out_wide, out_narrow, mlp_gain, up_weight, down_weight):
    gated_wide = group_output(query_wide, key_wide, value_wide, decay_wide, gate_wide, head_gain)
    gated_narrow = group_output(query_narrow, key_narrow, value_narrow, decay_narrow, gate_narrow, head_gain)
    mixed = blockwise_sum((gated_wide, gated_narrow), (out_wide, out_narrow))
    stream = (residual.astype(jnp.float32) + mixed).astype(jnp.bfloat16)
    stream_f = stream.astype(jnp.float32)
    normed = (stream_f * lax.rsqrt(lax.optimization_barrier(jnp.mean(jnp.square(stream_f), axis=1, keepdims=True)) + EPS) * mlp_gain).astype(jnp.bfloat16)
    hidden = jnp.square(jax.nn.relu(jnp.dot(normed, up_weight, preferred_element_type=jnp.float32))).astype(jnp.bfloat16)
    mlp_sum = blockwise_sum((hidden,), (down_weight,))
    return (stream_f + mlp_sum).astype(jnp.bfloat16)
```

```python
import functools
import jax
import jax.numpy as jnp
from jax import lax
from jax.experimental import pallas as pl
from jax.experimental.pallas import tpu as pltpu
from jax.sharding import PartitionSpec as P

HEADS = 4
EPS = 1e-05
DECAY_NORMALIZER = 16.0
MESH = pl.DeviceIdType.MESH
BF = jnp.bfloat16
F32 = jnp.float32
VM = pltpu.VMEM
DMA = pltpu.SemaphoreType.DMA
SCAN_CHUNKS = 2
ROW_CHUNKS = 4

NT = ((1,), (1,))
NN = ((1,), (0,))
TN = ((0,), (0,))


def dot(a, b, dims):
    return lax.dot_general(a, b, (dims, ((), ())), preferred_element_type=F32)


def span(i, size):
    return pl.ds(pl.multiple_of(i * size, size), size)


def layer_kernel(
    n,
    residual, qw, kw, vw, dw, gw, qn, kn, vn, dn, gn, gain, outw, outn, mgain, up, down,
    out,
    q_all, k_all, d_all, v_wide, v_narrow, g_wide, g_narrow, w_out, res, d_shard, weights,
    within_all, keys_all, snaps, offsets, total, state, local_w, local_n, carried,
    e1s, e1r, chain_s, chain_r, e2s, prefix,
    gated, partial, near_r, pair_s, cross_r, stream, normed, hidden,
    r1, mix, r2,
    load, ring_s, ring_v, e1_s, e1_v, ch_s, ch_v, e2_s, e2_v,
    na_s, na_v, cr_s, cr_v, st_s, st_v, s1, v1, s2, v2,
):
    s, t = lax.axis_index("sp"), lax.axis_index("tp")
    z, y = s // 2, lax.rem(s, 2)
    m, half_ring = n // 2, n // 2
    u = lax.rem(t, 2)
    near, far = t + 1 - 2 * u, lax.rem(t + 2, 4)
    cross = lax.rem(near + 2, 4)
    tokens, wide = qw.shape
    keys = wide + qn.shape[1]
    values = vw.shape[1]
    groups = ((0, wide, v_wide, local_w), (wide, keys, v_narrow, local_n))

    rows_chunk = tokens // ROW_CHUNKS
    half_rows = rows_chunk // 2
    shard_rows = up.shape[0]
    pairs = [
        (up, weights.at[0, span(s, shard_rows)]),
        (dw, d_all.at[:, :wide]), (dn, d_all.at[:, wide:]),
        (kw, k_all.at[:, :wide]), (kn, k_all.at[:, wide:]),
        (vw, v_wide), (vn, v_narrow),
        (down, d_shard),
        (qw, q_all.at[:, :wide]), (qn, q_all.at[:, wide:]),
        (gw, g_wide), (gn, g_narrow),
        (outw, w_out.at[:values]), (outn, w_out.at[values:]),
    ] + [
        (residual.at[pl.ds(pl.multiple_of(c * rows_chunk + u * half_rows, half_rows), half_rows)],
         res.at[c])
        for c in range(ROW_CHUNKS)
    ]
    loads = [
        pltpu.make_async_copy(a, b, load.at[i]) for i, (a, b) in enumerate(pairs)
    ]
    for copy in loads:
        copy.start()

    place = jnp.where(y == 0, z, n - 1 - z)

    def index_of(p):
        p = lax.rem(p + 2 * n, n)
        return jnp.where(p < m, 2 * p, 2 * (n - 1 - p) + 1)

    barrier = pltpu.get_barrier_semaphore()
    partner = s + 1 - 2 * y
    for other in (index_of(place + 1), index_of(place - 1), partner):
        pl.semaphore_signal(barrier, inc=1, device_id={"sp": other}, device_id_type=MESH)
    for other in (near, far):
        pl.semaphore_signal(barrier, inc=1, device_id={"tp": other}, device_id_type=MESH)
    pl.semaphore_wait(barrier, 5)

    cut = shard_rows // 2

    def hop_copy(kind, dist, first, side):
        way = lax.rem(side + y, 2)
        step = 1 - 2 * way
        piece = way if first else 1 - way
        origin = index_of(place - step * (dist - 1))
        rows = pl.ds(pl.multiple_of(origin * shard_rows + piece * cut, cut), cut)
        return pltpu.make_async_remote_copy(
            src_ref=weights.at[kind, rows], dst_ref=weights.at[kind, rows],
            send_sem=ring_s.at[kind, way, dist - 1, piece],
            recv_sem=ring_v.at[kind, way, dist - 1, piece],
            device_id={"sp": index_of(place + step)}, device_id_type=MESH,
        )

    def hop(kind, dist, first, side):
        if dist > 1:
            hop_copy(kind, dist - 1, first, side).wait_recv()
        hop_copy(kind, dist, first, side).start()

    def hops(kind, dist):
        for first in (True, False) if dist < half_ring else (True,):
            for side in (0, 1):
                hop(kind, dist, first, side)

    def arrive(kind):
        for side in (0, 1):
            hop_copy(kind, half_ring, True, side).wait_recv()
            if half_ring > 1:
                hop_copy(kind, half_ring - 1, False, side).wait_recv()

    loads[0].wait()
    hop(0, 1, True, 0)
    hop(0, 1, True, 1)

    block = min(128, tokens)
    blocks = tokens // block
    tril = lax.broadcasted_iota(jnp.int32, (block, block), 0) >= lax.broadcasted_iota(
        jnp.int32, (block, block), 1
    )
    ones = tril.astype(F32).astype(BF)
    total[...] = jnp.zeros_like(total)
    state[...] = jnp.zeros_like(state)
    for copy in loads[1:7]:
        copy.wait()

    def pass_one(i, carry):
        rows = span(i, block)
        decay = d_all[rows, :].astype(F32)
        g = (jnp.minimum(decay, 0.0) - jnp.log1p(jnp.exp(-jnp.abs(decay)))) / DECAY_NORMALIZER
        high = g.astype(BF)
        low = (g - high.astype(F32)).astype(BF)
        within = dot(ones, high, NN) + dot(ones, low, NN)
        within_all[rows, :] = within
        mid = within[block // 2 - 1 : block // 2]
        last = within[block - 1 : block]
        scaled = k_all[rows, :].astype(F32) * jnp.exp(mid - within)
        keys_all[rows, :] = scaled.astype(BF)
        ends = (scaled * jnp.exp(last - mid)).astype(BF)
        fade = jnp.exp(last)
        for lo, hi, v, _ in groups:
            before = state[:, lo:hi]
            snaps[i, :, lo:hi] = before.astype(BF)
            state[:, lo:hi] = before * fade[:, lo:hi] + dot(v[rows, :], ends[:, lo:hi], TN)
        offsets[i] = total[...]
        total[...] = total[...] + last
        return carry

    lax.fori_loop(0, blocks, pass_one, 0)

    half = values // 2
    part = half // SCAN_CHUNKS
    mine = jnp.exp(total[...])
    mine_high = mine.astype(BF)
    mine_low = (mine - mine_high.astype(F32)).astype(BF)
    e1s[:8, :] = jnp.broadcast_to(mine_high.astype(F32), (8, keys)).astype(BF)
    e1s[8:16, :] = jnp.broadcast_to(mine_low.astype(F32), (8, keys)).astype(BF)
    e1s[16:, :] = state[span(1 - y, half), :].astype(BF)

    def e1_copy(c):
        where = pl.ds(0, 16 + part) if c == 0 else pl.ds(16 + c * part, part)
        return pltpu.make_async_remote_copy(
            src_ref=e1s.at[where], dst_ref=e1r.at[where], send_sem=e1_s.at[c],
            recv_sem=e1_v.at[c], device_id={"sp": partner}, device_id_type=MESH,
        )

    def chain_copy(c):
        where = pl.ds(c * part, part)
        return pltpu.make_async_remote_copy(
            src_ref=chain_s.at[where], dst_ref=chain_r.at[where], send_sem=ch_s.at[c],
            recv_sem=ch_v.at[c], device_id={"sp": lax.rem(s + 2, n)}, device_id_type=MESH,
        )

    def e2_copy(c):
        return pltpu.make_async_remote_copy(
            src_ref=e2s.at[pl.ds(c * part, part)],
            dst_ref=prefix.at[pl.ds(pl.multiple_of(y * half + c * part, part), part)],
            send_sem=e2_s.at[c], recv_sem=e2_v.at[c], device_id={"sp": partner},
            device_id_type=MESH,
        )

    for c in range(SCAN_CHUNKS):
        e1_copy(c).start()

    hop(0, 1, False, 1)
    hop(0, 1, False, 0)
    loads[7].wait()
    weights[1, span(s, shard_rows), :] = d_shard[...].T
    hop(1, 1, True, 1)
    hop(1, 1, False, 1)
    early_a = z >= 1
    early_b = jnp.logical_and(z >= 2, z < m - 1)

    @pl.when(early_a)
    def _():
        hop(1, 1, True, 0)

    @pl.when(early_b)
    def _():
        hop(1, 1, False, 0)

    for copy in loads[8:10]:
        copy.wait()
    column = lax.broadcasted_iota(jnp.int32, (1, keys), 1)
    scale = jnp.where(column < wide, wide ** -0.5, (keys - wide) ** -0.5).astype(F32)

    def pass_two(i, carry):
        rows = span(i, block)
        within = within_all[rows, :]
        mid = within[block // 2 - 1 : block // 2]
        scaled = q_all[rows, :].astype(F32) * scale * jnp.exp(within - mid)
        whole = scaled * jnp.exp(mid)
        scaled = scaled.astype(BF)
        carried[rows, :] = (whole * jnp.exp(offsets[i])).astype(BF)
        whole = whole.astype(BF)
        for lo, hi, v, local in groups:
            scores = dot(scaled[:, lo:hi], keys_all[rows, lo:hi], NT)
            scores = jnp.where(tril, scores, 0.0).astype(BF)
            local[rows, :] = (
                dot(scores, v[rows, :], NN) + dot(whole[:, lo:hi], snaps[i, :, lo:hi], NT)
            ).astype(BF)
        return carry

    ahead = jnp.minimum(z * (blocks // 2), blocks)
    lax.fori_loop(0, ahead, pass_two, 0)

    @pl.when(z == 0)
    def _():
        chain_r[...] = jnp.zeros_like(chain_r)

    for c in range(SCAN_CHUNKS):
        e1_copy(c).wait_recv()

        @pl.when(z > 0)
        def _():
            chain_copy(c).wait_recv()

        other = e1r[:8, :].astype(F32)[:1] + e1r[8:16, :].astype(F32)[:1]
        fade_even = jnp.where(y == 0, mine, other)
        fade_odd = jnp.where(y == 0, other, mine)
        where = pl.ds(c * part, part)
        own = state[pl.ds(pl.multiple_of(y * half + c * part, part), part), :]
        theirs = e1r[16 + c * part : 16 + (c + 1) * part, :].astype(F32)
        even = jnp.where(y == 0, own, theirs)
        odd = jnp.where(y == 0, theirs, own)
        before = chain_r[where, :].astype(F32)
        between = before * fade_even + even
        chain_s[where, :] = (between * fade_odd + odd).astype(BF)

        @pl.when(z < m - 1)
        def _():
            chain_copy(c).start()

        prefix[pl.ds(pl.multiple_of(y * half + c * part, part), part), :] = jnp.where(
            y == 0, before, between
        ).astype(BF)
        e2s[where, :] = jnp.where(y == 0, between, before).astype(BF)
        e2_copy(c).start()

    @pl.when(jnp.logical_not(early_a))
    def _():
        hop(1, 1, True, 0)

    @pl.when(jnp.logical_not(early_b))
    def _():
        hop(1, 1, False, 0)

    lax.fori_loop(ahead, blocks, pass_two, 0)
    if half_ring >= 2:
        hops(0, 2)
        hops(1, 2)
    for copy in loads[10:]:
        copy.wait()
    for c in range(SCAN_CHUNKS):
        e2_copy(c).wait_recv()

    def near_copy(c):
        return pltpu.make_async_remote_copy(
            src_ref=partial.at[
                pl.ds(pl.multiple_of(c * rows_chunk + (1 - u) * half_rows, half_rows), half_rows)
            ],
            dst_ref=near_r.at[c], send_sem=na_s.at[c], recv_sem=na_v.at[c],
            device_id={"tp": near}, device_id_type=MESH,
        )

    def cross_copy(c):
        return pltpu.make_async_remote_copy(
            src_ref=pair_s.at[c], dst_ref=cross_r.at[c], send_sem=cr_s.at[c],
            recv_sem=cr_v.at[c], device_id={"tp": far}, device_id_type=MESH,
        )

    def own_rows(c):
        return pl.ds(pl.multiple_of(c * rows_chunk + u * half_rows, half_rows), half_rows)

    def other_rows(c):
        return pl.ds(
            pl.multiple_of(c * rows_chunk + (1 - u) * half_rows, half_rows), half_rows
        )

    def stream_copy(c):
        return pltpu.make_async_remote_copy(
            src_ref=stream.at[own_rows(c)], dst_ref=stream.at[own_rows(c)],
            send_sem=st_s.at[c], recv_sem=st_v.at[c],
            device_id={"tp": near}, device_id_type=MESH,
        )

    width = w_out.shape[1]
    tile = min(512, width)

    def project(c, carry):
        rows = span(c, rows_chunk)
        for j, (lo, hi, _, local) in enumerate(groups):
            gate = (g_wide, g_narrow)[j]
            x = local[rows, :].astype(F32) + dot(carried[rows, lo:hi], prefix[:, lo:hi], NT)
            fit = lax.rsqrt(jnp.mean(jnp.square(x), axis=-1, keepdims=True) + EPS)
            v = gate[rows, :].astype(F32)
            gated[:, j * values : (j + 1) * values] = (
                x * fit * gain[...] * (v / (1.0 + jnp.exp(-v)))
            ).astype(BF)
        for lo in range(0, width, tile):
            partial[rows, lo : lo + tile] = dot(
                gated[...], w_out[:, lo : lo + tile], NN
            ).astype(BF)
        near_copy(c).start()

        @pl.when(c > 0)
        def _():
            pair(c - 1)

        return carry

    def pair(c):
        near_copy(c).wait_recv()
        pair_s[c] = (partial[own_rows(c), :].astype(F32) + near_r[c].astype(F32)).astype(BF)
        cross_copy(c).start()

    lax.fori_loop(0, ROW_CHUNKS, project, 0)
    pair(ROW_CHUNKS - 1)

    def norm(rows):
        x = stream[rows, :].astype(F32)
        fit = lax.rsqrt(jnp.mean(jnp.square(x), axis=1, keepdims=True) + EPS)
        normed[rows, :] = (x * fit * mgain[...]).astype(BF)

    def settle(c):
        cross_copy(c).wait_recv()
        value = pair_s[c].astype(F32) + cross_r[c].astype(F32)
        stream[own_rows(c), :] = (res[c].astype(F32) + value).astype(BF)
        stream_copy(c).start()
        norm(own_rows(c))
        stream_copy(c).wait_recv()
        norm(other_rows(c))

    inner = up.shape[1]
    tile_h = min(512, inner)

    def expand(c, carry):
        rows = span(c, rows_chunk)
        for lo in range(0, inner, tile_h):
            h = dot(normed[rows, :], weights[0, :, lo : lo + tile_h], NN)
            hidden[rows, lo : lo + tile_h] = jnp.square(jnp.maximum(h, 0.0)).astype(BF)
        return carry

    for dist in range(3, half_ring):
        hops(0, dist)
    settle(0)
    settle(1)
    if half_ring >= 3:
        hops(0, half_ring)
    for dist in range(3, half_ring):
        hops(1, dist)
    settle(2)
    arrive(0)
    lax.fori_loop(0, 3, expand, 0)
    settle(3)
    if half_ring >= 3:
        hops(1, half_ring)
    expand(3, 0)
    arrive(1)
    for c in range(ROW_CHUNKS):
        near_copy(c).wait_send()

    own_width = out.shape[1]

    def cols(owner):
        return span(owner, own_width)

    def first(which, c):
        return pltpu.make_async_remote_copy(
            src_ref=partial.at[span(c, rows_chunk), cols((near, cross)[which])],
            dst_ref=r1.at[which, c], send_sem=s1.at[which, c], recv_sem=v1.at[which, c],
            device_id={"tp": near}, device_id_type=MESH,
        )

    def second(c):
        return pltpu.make_async_remote_copy(
            src_ref=mix.at[c], dst_ref=r2.at[c], send_sem=s2.at[c], recv_sem=v2.at[c],
            device_id={"tp": far}, device_id_type=MESH,
        )

    def across(c):
        first(1, c).wait_recv()
        rows = span(c, rows_chunk)
        mix[c] = (partial[rows, cols(far)].astype(F32) + r1[1, c].astype(F32)).astype(BF)
        second(c).start()

    def contract(c, carry):
        rows = span(c, rows_chunk)
        for lo in range(0, width, tile):
            partial[rows, lo : lo + tile] = dot(
                hidden[rows, :], weights[1, lo : lo + tile, :], NT
            ).astype(BF)
        first(1, c).start()
        first(0, c).start()

        @pl.when(c > 0)
        def _():
            across(c - 1)

        return carry

    lax.fori_loop(0, ROW_CHUNKS, contract, 0)
    across(ROW_CHUNKS - 1)

    def close(c, carry):
        first(0, c).wait_recv()
        second(c).wait_recv()
        rows = span(c, rows_chunk)
        value = partial[rows, cols(t)].astype(F32) + r1[0, c].astype(F32) + r2[c].astype(F32)
        out[rows, :] = (stream[rows, cols(t)].astype(F32) + value).astype(BF)
        first(0, c).wait_send()
        first(1, c).wait_send()
        second(c).wait_send()
        return carry

    lax.fori_loop(0, ROW_CHUNKS, close, 0)

    for c in range(SCAN_CHUNKS):
        e1_copy(c).wait_send()
        e2_copy(c).wait_send()

        @pl.when(z < m - 1)
        def _():
            chain_copy(c).wait_send()

    for c in range(ROW_CHUNKS):
        cross_copy(c).wait_send()
        stream_copy(c).wait_send()
    for kind in (0, 1):
        for dist in range(1, half_ring + 1):
            for is_first in (True, False) if dist < half_ring else (True,):
                for side in (0, 1):
                    hop_copy(kind, dist, is_first, side).wait_send()


def layer(n, *args):
    (residual, qw, kw, vw, dw, gw, qn, kn, vn, dn, gn, gain, outw, outn, mgain, up, down) = args
    tokens, wide = qw.shape
    keys = wide + qn.shape[1]
    values = vw.shape[1]
    width = outw.shape[1]
    inner = up.shape[1]
    own_width = width // 4
    block = min(128, tokens)
    blocks = tokens // block
    rc = tokens // ROW_CHUNKS
    hr = rc // 2
    anyspace = pl.BlockSpec(memory_space=pl.ANY)
    vspace = pl.BlockSpec(memory_space=VM)
    half = values // 2
    scratch = [
        VM((tokens, keys), BF), VM((tokens, keys), BF), VM((tokens, keys), BF),
        VM((tokens, values), BF), VM((tokens, values), BF),
        VM((tokens, values), BF), VM((tokens, values), BF),
        VM((2 * values, width), BF), VM((ROW_CHUNKS, hr, width), BF),
        VM(down.shape, BF), VM((2, n * up.shape[0], inner), BF),
        VM((tokens, keys), F32), VM((tokens, keys), BF), VM((blocks, values, keys), BF),
        VM((blocks, 1, keys), F32), VM((1, keys), F32), VM((values, keys), F32),
        VM((tokens, values), BF), VM((tokens, values), BF), VM((tokens, keys), BF),
        VM((16 + half, keys), BF), VM((16 + half, keys), BF),
        VM((half, keys), BF), VM((half, keys), BF), VM((half, keys), BF),
        VM((values, keys), BF),
        VM((rc, 2 * values), BF), VM((tokens, width), BF),
        VM((ROW_CHUNKS, hr, width), BF), VM((ROW_CHUNKS, hr, width), BF),
        VM((ROW_CHUNKS, hr, width), BF),
        VM((tokens, width), BF), VM((tokens, width), BF), VM((tokens, inner), BF),
        VM((2, ROW_CHUNKS, rc, own_width), BF), VM((ROW_CHUNKS, rc, own_width), BF),
        VM((ROW_CHUNKS, rc, own_width), BF),
        DMA((14 + ROW_CHUNKS,)),
        DMA((2, 2, n // 2, 2)), DMA((2, 2, n // 2, 2)),
    ] + [DMA((SCAN_CHUNKS,))] * 6 + [DMA((ROW_CHUNKS,))] * 6 + [
        DMA((2, ROW_CHUNKS)), DMA((2, ROW_CHUNKS)), DMA((ROW_CHUNKS,)), DMA((ROW_CHUNKS,)),
    ]
    in_specs = [anyspace] * 17
    in_specs[11] = in_specs[14] = vspace
    return pl.pallas_call(
        functools.partial(layer_kernel, n),
        out_shape=jax.ShapeDtypeStruct((tokens, own_width), BF),
        in_specs=in_specs,
        out_specs=vspace,
        scratch_shapes=scratch,
        compiler_params=pltpu.CompilerParams(
            collective_id=0, has_side_effects=True, vmem_limit_bytes=63 * 2**20
        ),
        cost_estimate=pl.CostEstimate(
            flops=30 * 10**9, bytes_accessed=32 * 2**20, transcendentals=0
        ),
        name="layer",
    )(*args)


def body(*args):
    n_sp, n_tp = lax.axis_size("sp"), lax.axis_size("tp")
    assert n_tp == HEADS == 4 and n_sp % 2 == 0
    args = list(args)
    args[11] = args[11].reshape(1, -1)
    args[14] = args[14].reshape(1, -1)
    return layer(n_sp, *args)


def solution(mesh):
    return jax.shard_map(
        body,
        mesh=mesh,
        in_specs=(
            P("sp", None),
            P("sp", "tp"),
            P("sp", "tp"),
            P("sp", "tp"),
            P("sp", "tp"),
            P("sp", "tp"),
            P("sp", "tp"),
            P("sp", "tp"),
            P("sp", "tp"),
            P("sp", "tp"),
            P("sp", "tp"),
            P(),
            P("tp", None),
            P("tp", None),
            P(),
            P("sp", "tp"),
            P("tp", "sp"),
        ),
        out_specs=P("sp", "tp"),
        check_vma=False,
    )
```

```python
import functools
import jax
import jax.numpy as jnp
from jax import lax
from jax.experimental import pallas as pl
from jax.experimental.pallas import tpu as pltpu
from jax.sharding import PartitionSpec as P

HEADS = 4
EPS = 1e-05
DECAY_NORMALIZER = 16.0
MESH = pl.DeviceIdType.MESH
BF = jnp.bfloat16
F32 = jnp.float32
VM = pltpu.VMEM
DMA = pltpu.SemaphoreType.DMA
SCAN_CHUNKS = 4
ROW_CHUNKS = 8
EXPAND_CHUNKS = 4

NT = ((1,), (1,))
NN = ((1,), (0,))
TN = ((0,), (0,))


def dot(a, b, dims):
    return lax.dot_general(a, b, (dims, ((), ())), preferred_element_type=F32)


def span(i, size):
    return pl.ds(i * size if isinstance(i, int) else pl.multiple_of(i * size, size), size)


def layer_kernel(
    n,
    residual, qw, kw, vw, dw, gw, qn, kn, vn, dn, gn, gain, outw, outn, mgain, up, down,
    out,
    q_all, k_all, d_all, v_wide, v_narrow, g_wide, g_narrow, w_out, res, d_shard, weights,
    within_all, keys_all, snaps, offsets, total, state, local_w, local_n, carried,
    e1s, e1r, chain_s, chain_r, e2s, prefix,
    gated, partial, near_r, pair_s, cross_r, stream, normed, hidden,
    r1, mix, r2,
    load, ring_s, ring_v, e1_s, e1_v, ch_s, ch_v, e2_s, e2_v,
    na_s, na_v, cr_s, cr_v, st_s, st_v, s1, v1, s2, v2,
):
    s, t = lax.axis_index("sp"), lax.axis_index("tp")
    z, y = s // 2, lax.rem(s, 2)
    m, half_ring = n // 2, n // 2
    u = lax.rem(t, 2)
    near, far = t + 1 - 2 * u, lax.rem(t + 2, 4)
    cross = lax.rem(near + 2, 4)
    tokens, wide = qw.shape
    keys = wide + qn.shape[1]
    values = vw.shape[1]
    groups = ((0, wide, v_wide, local_w), (wide, keys, v_narrow, local_n))

    rows_chunk = tokens // ROW_CHUNKS
    half_rows = rows_chunk // 2
    shard_rows = up.shape[0]
    pairs = [
        (up, weights.at[0, span(s, shard_rows)]),
        (dw, d_all.at[:, :wide]), (dn, d_all.at[:, wide:]),
        (kw, k_all.at[:, :wide]), (kn, k_all.at[:, wide:]),
        (vw, v_wide), (vn, v_narrow),
        (down, d_shard),
        (qw, q_all.at[:, :wide]), (qn, q_all.at[:, wide:]),
        (gw, g_wide), (gn, g_narrow),
        (outw, w_out.at[:values]), (outn, w_out.at[values:]),
    ] + [
        (residual.at[pl.ds(pl.multiple_of(c * rows_chunk + u * half_rows, half_rows), half_rows)],
         res.at[c])
        for c in range(ROW_CHUNKS)
    ]
    loads = [
        pltpu.make_async_copy(a, b, load.at[i]) for i, (a, b) in enumerate(pairs)
    ]
    for copy in loads:
        copy.start()

    total[...] = jnp.zeros_like(total)
    state[...] = jnp.zeros_like(state)

    place = jnp.where(y == 0, z, n - 1 - z)

    def index_of(p):
        p = lax.rem(p + 2 * n, n)
        return jnp.where(p < m, 2 * p, 2 * (n - 1 - p) + 1)

    barrier = pltpu.get_barrier_semaphore()
    partner = s + 1 - 2 * y
    for other in (index_of(place + 1), index_of(place - 1), partner):
        pl.semaphore_signal(barrier, inc=1, device_id={"sp": other}, device_id_type=MESH)
    for other in (near, far):
        pl.semaphore_signal(barrier, inc=1, device_id={"tp": other}, device_id_type=MESH)
    pl.semaphore_wait(barrier, 5)

    cut = shard_rows // 2

    def hop_copy(kind, dist, first, side):
        way = lax.rem(side + y, 2)
        step = 1 - 2 * way
        piece = way if first else 1 - way
        origin = index_of(place - step * (dist - 1))
        rows = pl.ds(pl.multiple_of(origin * shard_rows + piece * cut, cut), cut)
        return pltpu.make_async_remote_copy(
            src_ref=weights.at[kind, rows], dst_ref=weights.at[kind, rows],
            send_sem=ring_s.at[kind, way, dist - 1, piece],
            recv_sem=ring_v.at[kind, way, dist - 1, piece],
            device_id={"sp": index_of(place + step)}, device_id_type=MESH,
        )

    def hop(kind, dist, first, side):
        if dist > 1:
            hop_copy(kind, dist - 1, first, side).wait_recv()
        hop_copy(kind, dist, first, side).start()

    def hops(kind, dist):
        for first in (True, False) if dist < half_ring else (True,):
            for side in (0, 1):
                hop(kind, dist, first, side)

    def arrive(kind):
        for side in (0, 1):
            hop_copy(kind, half_ring, True, side).wait_recv()
            if half_ring > 1:
                hop_copy(kind, half_ring - 1, False, side).wait_recv()

    loads[0].wait()
    hop(0, 1, True, 0)
    hop(0, 1, True, 1)

    block = min(128, tokens)
    blocks = tokens // block
    tril = lax.broadcasted_iota(jnp.int32, (block, block), 0) >= lax.broadcasted_iota(
        jnp.int32, (block, block), 1
    )
    ones = tril.astype(F32).astype(BF)
    for copy in loads[1:7]:
        copy.wait()

    def pass_one(i, carry):
        rows = span(i, block)
        decay = d_all[rows, :].astype(F32)
        g = (jnp.minimum(decay, 0.0) - jnp.log(1.0 + jnp.exp(-jnp.abs(decay)))) / DECAY_NORMALIZER
        high = g.astype(BF)
        low = (g - high.astype(F32)).astype(BF)
        within = dot(ones, high, NN) + dot(ones, low, NN)
        within_all[rows, :] = within
        mid = within[block // 2 - 1 : block // 2]
        last = within[block - 1 : block]
        scaled = k_all[rows, :].astype(F32) * jnp.exp(mid - within)
        keys_all[rows, :] = scaled.astype(BF)
        ends = (scaled * jnp.exp(last - mid)).astype(BF)
        fade = jnp.exp(last)
        for lo, hi, v, _ in groups:
            before = state[:, lo:hi]
            snaps[i, :, lo:hi] = before.astype(BF)
            state[:, lo:hi] = before * fade[:, lo:hi] + dot(v[rows, :], ends[:, lo:hi], TN)
        offsets[i] = total[...]
        total[...] = total[...] + last
        return carry

    lax.fori_loop(0, blocks, pass_one, 0)

    half = values // 2
    part = half // SCAN_CHUNKS
    mine = jnp.exp(total[...])
    mine_high = mine.astype(BF)
    mine_low = (mine - mine_high.astype(F32)).astype(BF)
    e1s[:8, :] = jnp.broadcast_to(mine_high.astype(F32), (8, keys)).astype(BF)
    e1s[8:16, :] = jnp.broadcast_to(mine_low.astype(F32), (8, keys)).astype(BF)
    e1s[16:, :] = state[span(1 - y, half), :].astype(BF)

    def e1_copy(c):
        where = pl.ds(0, 16 + part) if c == 0 else pl.ds(16 + c * part, part)
        return pltpu.make_async_remote_copy(
            src_ref=e1s.at[where], dst_ref=e1r.at[where], send_sem=e1_s.at[c],
            recv_sem=e1_v.at[c], device_id={"sp": partner}, device_id_type=MESH,
        )

    def chain_copy(c):
        where = pl.ds(c * part, part)
        return pltpu.make_async_remote_copy(
            src_ref=chain_s.at[where], dst_ref=chain_r.at[where], send_sem=ch_s.at[c],
            recv_sem=ch_v.at[c], device_id={"sp": lax.rem(s + 2, n)}, device_id_type=MESH,
        )

    def e2_copy(c):
        return pltpu.make_async_remote_copy(
            src_ref=e2s.at[pl.ds(c * part, part)],
            dst_ref=prefix.at[pl.ds(pl.multiple_of(y * half + c * part, part), part)],
            send_sem=e2_s.at[c], recv_sem=e2_v.at[c], device_id={"sp": partner},
            device_id_type=MESH,
        )

    for c in range(SCAN_CHUNKS):
        e1_copy(c).start()

    hop(0, 1, False, 1)
    hop(0, 1, False, 0)
    loads[7].wait()
    weights[1, span(s, shard_rows), :] = d_shard[...].T
    inner_pair = z > 0
    early_a = z >= 2

    @pl.when(inner_pair)
    def _():
        hop(1, 1, True, 1)
        hop(1, 1, False, 1)

    @pl.when(early_a)
    def _():
        hop(1, 1, True, 0)

    for copy in loads[8:10]:
        copy.wait()
    column = lax.broadcasted_iota(jnp.int32, (1, keys), 1)
    scale = jnp.where(column < wide, wide ** -0.5, (keys - wide) ** -0.5).astype(F32)

    def pass_two(i, carry):
        rows = span(i, block)
        within = within_all[rows, :]
        mid = within[block // 2 - 1 : block // 2]
        scaled = q_all[rows, :].astype(F32) * scale * jnp.exp(within - mid)
        whole = scaled * jnp.exp(mid)
        scaled = scaled.astype(BF)
        carried[rows, :] = (whole * jnp.exp(offsets[i])).astype(BF)
        whole = whole.astype(BF)
        for lo, hi, v, local in groups:
            scores = dot(scaled[:, lo:hi], keys_all[rows, lo:hi], NT)
            scores = jnp.where(tril, scores, 0.0).astype(BF)
            local[rows, :] = (
                dot(scores, v[rows, :], NN) + dot(whole[:, lo:hi], snaps[i, :, lo:hi], NT)
            ).astype(BF)
        return carry

    ahead = jnp.minimum(z * (blocks // 2), blocks)
    lax.fori_loop(0, ahead, pass_two, 0)

    @pl.when(z == 0)
    def _():
        chain_r[...] = jnp.zeros_like(chain_r)

    for c in range(SCAN_CHUNKS):
        e1_copy(c).wait_recv()

        @pl.when(z > 0)
        def _():
            chain_copy(c).wait_recv()

        other = e1r[:8, :].astype(F32)[:1] + e1r[8:16, :].astype(F32)[:1]
        fade_even = jnp.where(y == 0, mine, other)
        fade_odd = jnp.where(y == 0, other, mine)
        where = pl.ds(c * part, part)
        own = state[pl.ds(pl.multiple_of(y * half + c * part, part), part), :]
        theirs = e1r[16 + c * part : 16 + (c + 1) * part, :].astype(F32)
        even = jnp.where(y == 0, own, theirs)
        odd = jnp.where(y == 0, theirs, own)
        before = chain_r[where, :].astype(F32)
        between = before * fade_even + even
        chain_s[where, :] = (between * fade_odd + odd).astype(BF)

        @pl.when(z < m - 1)
        def _():
            chain_copy(c).start()

        prefix[pl.ds(pl.multiple_of(y * half + c * part, part), part), :] = jnp.where(
            y == 0, before, between
        ).astype(BF)
        e2s[where, :] = jnp.where(y == 0, between, before).astype(BF)
        e2_copy(c).start()

    @pl.when(jnp.logical_not(inner_pair))
    def _():
        hop(1, 1, True, 1)
        hop(1, 1, False, 1)

    @pl.when(jnp.logical_not(early_a))
    def _():
        hop(1, 1, True, 0)

    hop(1, 1, False, 0)

    lax.fori_loop(ahead, blocks, pass_two, 0)
    for copy in loads[10:]:
        copy.wait()
    for c in range(SCAN_CHUNKS):
        e2_copy(c).wait_recv()
    if half_ring >= 2:
        hops(0, 2)

    def near_copy(c):
        return pltpu.make_async_remote_copy(
            src_ref=partial.at[
                pl.ds(pl.multiple_of(c * rows_chunk + (1 - u) * half_rows, half_rows), half_rows)
            ],
            dst_ref=near_r.at[c], send_sem=na_s.at[c], recv_sem=na_v.at[c],
            device_id={"tp": near}, device_id_type=MESH,
        )

    def cross_copy(c):
        return pltpu.make_async_remote_copy(
            src_ref=pair_s.at[c], dst_ref=cross_r.at[c], send_sem=cr_s.at[c],
            recv_sem=cr_v.at[c], device_id={"tp": far}, device_id_type=MESH,
        )

    def own_rows(c):
        return pl.ds(pl.multiple_of(c * rows_chunk + u * half_rows, half_rows), half_rows)

    def other_rows(c):
        return pl.ds(
            pl.multiple_of(c * rows_chunk + (1 - u) * half_rows, half_rows), half_rows
        )

    def stream_copy(c):
        return pltpu.make_async_remote_copy(
            src_ref=stream.at[own_rows(c)], dst_ref=stream.at[own_rows(c)],
            send_sem=st_s.at[c], recv_sem=st_v.at[c],
            device_id={"tp": near}, device_id_type=MESH,
        )

    width = w_out.shape[1]
    tile = min(512, width)

    def project(c, carry):
        rows = span(c, rows_chunk)
        for j, (lo, hi, _, local) in enumerate(groups):
            gate = (g_wide, g_narrow)[j]
            x = local[rows, :].astype(F32) + dot(carried[rows, lo:hi], prefix[:, lo:hi], NT)
            fit = lax.rsqrt(jnp.mean(jnp.square(x), axis=-1, keepdims=True) + EPS)
            v = gate[rows, :].astype(F32)
            gated[:, j * values : (j + 1) * values] = (
                x * fit * gain[...] * (v / (1.0 + jnp.exp(-v)))
            ).astype(BF)
        for lo in range(0, width, tile):
            partial[rows, lo : lo + tile] = dot(
                gated[...], w_out[:, lo : lo + tile], NN
            ).astype(BF)
        near_copy(c).start()

        @pl.when(c > 0)
        def _():
            pair(c - 1)

        return carry

    def pair(c):
        near_copy(c).wait_recv()
        pair_s[c] = (partial[own_rows(c), :].astype(F32) + near_r[c].astype(F32)).astype(BF)
        cross_copy(c).start()

    lax.fori_loop(0, ROW_CHUNKS, project, 0)
    pair(ROW_CHUNKS - 1)

    def norm(rows):
        x = stream[rows, :].astype(F32)
        fit = lax.rsqrt(jnp.mean(jnp.square(x), axis=1, keepdims=True) + EPS)
        normed[rows, :] = (x * fit * mgain[...]).astype(BF)

    def settle(c):
        cross_copy(c).wait_recv()
        value = pair_s[c].astype(F32) + cross_r[c].astype(F32)
        stream[own_rows(c), :] = (res[c].astype(F32) + value).astype(BF)
        stream_copy(c).start()
        norm(own_rows(c))
        stream_copy(c).wait_recv()
        norm(other_rows(c))

    inner = up.shape[1]
    tile_h = min(512, inner)

    def expand(c, carry):
        rows = span(c, tokens // EXPAND_CHUNKS)
        for lo in range(0, inner, tile_h):
            h = dot(normed[rows, :], weights[0, :, lo : lo + tile_h], NN)
            hidden[rows, lo : lo + tile_h] = jnp.square(jnp.maximum(h, 0.0)).astype(BF)
        return carry

    later = []
    for dist in range(2, half_ring + 1):
        group = [(1, dist, True), (0, dist + 1, True), (0, dist + 1, False), (1, dist, False)]
        if dist > 2:
            group[0], group[1] = group[1], group[0]
        later += [h for h in group if h[1] < half_ring or (h[1] == half_ring and h[2])]
    points = (0, 0, 2, 2, 4, 4, 6, ROW_CHUNKS + 1)
    each = -(-len(later) // 6)
    due = [points[i] if half_ring <= 4 else i // each for i in range(len(later))]

    def serve(point):
        for (kind, dist, is_first), at in zip(later, due):
            if at == point:
                for side in (0, 1):
                    hop(kind, dist, is_first, side)

    own_width = out.shape[1]
    by_shard = shard_rows >= 128 and half_ring >= 3
    shard = shard_rows if by_shard else max(shard_rows, 128)
    shards = width // shard
    per = own_width // shard
    tall = tokens // 2
    if by_shard:
        near_by = 2 * (half_ring - 2) + 1
        first_part = [near_by - 1, near_by - 2] + list(range(near_by - 2))
        table = [(k, 0) for k in first_part]
        table += [(near_by, 0), (near_by, 1), (first_part[0], 1), (first_part[1], 1)]
        table += [(near_by + 1, 0), (near_by + 1, 1)] + [(k, 1) for k in first_part[2:]]
        table += [(near_by + 2, 0), (near_by + 2, 1)]
    else:
        table = [(k, h) for h in (0, 1) for k in range(shards)]

    def look(i, column):
        value = table[0][column]
        for n_row, row in enumerate(table[1:], 1):
            value = jnp.where(i == n_row, row[column], value)
        return value

    def place_of(i):
        k, h = look(i, 0), look(i, 1)
        if by_shard:
            dist = (k + 1) // 2
            k = index_of(place + jnp.where(lax.rem(k, 2) == 1, dist, -dist))
        return k, lax.rem(k, per), k // per, h

    def to_near(which, q, j, h):
        return pltpu.make_async_remote_copy(
            src_ref=partial.at[span(h, tall), span(j, shard)],
            dst_ref=r1.at[which, q, span(h, tall)],
            send_sem=s1.at[which, q, h], recv_sem=v1.at[which, q, h],
            device_id={"tp": near}, device_id_type=MESH,
        )

    def to_far(q, h):
        return pltpu.make_async_remote_copy(
            src_ref=mix.at[q, span(h, tall)], dst_ref=r2.at[q, span(h, tall)],
            send_sem=s2.at[q, h], recv_sem=v2.at[q, h],
            device_id={"tp": far}, device_id_type=MESH,
        )

    def across(i):
        j, q, owner, h = place_of(i)

        @pl.when(owner == far)
        def _():
            to_near(1, q, j, h).wait_recv()
            rows = span(h, tall)
            mix[q, rows] = (
                partial[rows, span(j, shard)].astype(F32) + r1[1, q, rows].astype(F32)
            ).astype(BF)
            to_far(q, h).start()

    def contract(begin, i, carry):
        j, q, owner, h = place_of(i)
        rows = span(h, tall)
        partial[rows, span(j, shard)] = dot(
            hidden[rows, :], weights[1, span(j, shard), :], NT
        ).astype(BF)

        @pl.when(owner == near)
        def _():
            to_near(0, q, j, h).start()

        @pl.when(owner == cross)
        def _():
            to_near(1, q, j, h).start()

        @pl.when(i > begin)
        def _():
            across(i - 1)

        return carry

    def contract_all(begin, end):
        lax.fori_loop(begin, end, functools.partial(contract, begin), 0)
        across(end - 1)

    serve(0)
    per_expand = ROW_CHUNKS // EXPAND_CHUNKS
    for c in range(ROW_CHUNKS):
        settle(c)
        serve(c + 1)
        if c == ROW_CHUNKS - per_expand - 1:
            arrive(0)
            lax.fori_loop(0, EXPAND_CHUNKS // 2, expand, 0)
            for i in range(ROW_CHUNKS):
                near_copy(i).wait_send()
            if by_shard:
                contract_all(0, near_by)
            serve(ROW_CHUNKS + 1)
            lax.fori_loop(EXPAND_CHUNKS // 2, EXPAND_CHUNKS - 1, expand, 0)
    expand(EXPAND_CHUNKS - 1, 0)
    if by_shard:
        for side in (0, 1):
            hop_copy(1, half_ring - 1, False, side).wait_recv()
        contract_all(near_by, len(table) - 2)
        for side in (0, 1):
            hop_copy(1, half_ring, True, side).wait_recv()
        contract_all(len(table) - 2, len(table))
    else:
        arrive(1)
        contract_all(0, len(table))

    for h in (0, 1):
        for q in range(per):
            j = t * per + q
            rows = span(h, tall)
            to_near(0, q, j, h).wait_recv()
            to_far(q, h).wait_recv()
            value = partial[rows, span(j, shard)].astype(F32) + r1[0, q, rows].astype(F32)
            value = value + r2[q, rows].astype(F32)
            out[rows, q * shard : (q + 1) * shard] = (
                stream[rows, span(j, shard)].astype(F32) + value
            ).astype(BF)
    for q in range(per):
        for h in (0, 1):
            to_near(0, q, near * per + q, h).wait_send()
            to_near(1, q, cross * per + q, h).wait_send()
            to_far(q, h).wait_send()

    for c in range(SCAN_CHUNKS):
        e1_copy(c).wait_send()
        e2_copy(c).wait_send()

        @pl.when(z < m - 1)
        def _():
            chain_copy(c).wait_send()

    for c in range(ROW_CHUNKS):
        cross_copy(c).wait_send()
        stream_copy(c).wait_send()
    for kind in (0, 1):
        for dist in range(1, half_ring + 1):
            for is_first in (True, False) if dist < half_ring else (True,):
                for side in (0, 1):
                    hop_copy(kind, dist, is_first, side).wait_send()


def layer(n, *args):
    (residual, qw, kw, vw, dw, gw, qn, kn, vn, dn, gn, gain, outw, outn, mgain, up, down) = args
    tokens, wide = qw.shape
    keys = wide + qn.shape[1]
    values = vw.shape[1]
    width = outw.shape[1]
    inner = up.shape[1]
    own_width = width // 4
    block = min(128, tokens)
    blocks = tokens // block
    rc = tokens // ROW_CHUNKS
    hr = rc // 2
    anyspace = pl.BlockSpec(memory_space=pl.ANY)
    vspace = pl.BlockSpec(memory_space=VM)
    half = values // 2
    shard = max(down.shape[1], 128)
    per = own_width // shard
    scratch = [
        VM((tokens, keys), BF), VM((tokens, keys), BF), VM((tokens, keys), BF),
        VM((tokens, values), BF), VM((tokens, values), BF),
        VM((tokens, values), BF), VM((tokens, values), BF),
        VM((2 * values, width), BF), VM((ROW_CHUNKS, hr, width), BF),
        VM(down.shape, BF), VM((2, n * up.shape[0], inner), BF),
        VM((tokens, keys), F32), VM((tokens, keys), BF), VM((blocks, values, keys), BF),
        VM((blocks, 1, keys), F32), VM((1, keys), F32), VM((values, keys), F32),
        VM((tokens, values), BF), VM((tokens, values), BF), VM((tokens, keys), BF),
        VM((16 + half, keys), BF), VM((16 + half, keys), BF),
        VM((half, keys), BF), VM((half, keys), BF), VM((half, keys), BF),
        VM((values, keys), BF),
        VM((rc, 2 * values), BF), VM((tokens, width), BF),
        VM((ROW_CHUNKS, hr, width), BF), VM((ROW_CHUNKS, hr, width), BF),
        VM((ROW_CHUNKS, hr, width), BF),
        VM((tokens, width), BF), VM((tokens, width), BF), VM((tokens, inner), BF),
        VM((2, per, tokens, shard), BF), VM((per, tokens, shard), BF),
        VM((per, tokens, shard), BF),
        DMA((14 + ROW_CHUNKS,)),
        DMA((2, 2, n // 2, 2)), DMA((2, 2, n // 2, 2)),
    ] + [DMA((SCAN_CHUNKS,))] * 6 + [DMA((ROW_CHUNKS,))] * 6 + [
        DMA((2, per, 2)), DMA((2, per, 2)), DMA((per, 2)), DMA((per, 2)),
    ]
    in_specs = [anyspace] * 17
    in_specs[11] = in_specs[14] = vspace
    return pl.pallas_call(
        functools.partial(layer_kernel, n),
        out_shape=jax.ShapeDtypeStruct((tokens, own_width), BF),
        in_specs=in_specs,
        out_specs=vspace,
        scratch_shapes=scratch,
        compiler_params=pltpu.CompilerParams(
            collective_id=0, has_side_effects=True, vmem_limit_bytes=63 * 2**20
        ),
        cost_estimate=pl.CostEstimate(
            flops=30 * 10**9, bytes_accessed=32 * 2**20, transcendentals=0
        ),
        name="layer",
    )(*args)


def body(*args):
    n_sp, n_tp = lax.axis_size("sp"), lax.axis_size("tp")
    assert n_tp == HEADS == 4 and n_sp % 2 == 0
    args = list(args)
    args[11] = args[11].reshape(1, -1)
    args[14] = args[14].reshape(1, -1)
    return layer(n_sp, *args)


def solution(mesh):
    return jax.shard_map(
        body,
        mesh=mesh,
        in_specs=(
            P("sp", None),
            P("sp", "tp"),
            P("sp", "tp"),
            P("sp", "tp"),
            P("sp", "tp"),
            P("sp", "tp"),
            P("sp", "tp"),
            P("sp", "tp"),
            P("sp", "tp"),
            P("sp", "tp"),
            P("sp", "tp"),
            P(),
            P("tp", None),
            P("tp", None),
            P(),
            P("sp", "tp"),
            P("tp", "sp"),
        ),
        out_specs=P("sp", "tp"),
        check_vma=False,
    )
```

```python
import functools
import jax
import jax.numpy as jnp
from jax import lax
from jax.experimental import pallas as pl
from jax.experimental.pallas import tpu as pltpu
from jax.sharding import PartitionSpec as P

HEADS = 4
EPS = 1e-05
DECAY_NORMALIZER = 16.0
MESH = pl.DeviceIdType.MESH
BF = jnp.bfloat16
F32 = jnp.float32
VM = pltpu.VMEM
DMA = pltpu.SemaphoreType.DMA
SCAN_CHUNKS = 8
ROW_CHUNKS = 8
EXPAND_CHUNKS = 4
POINTS = (0, 0, 2, 4, 3, 5, 7, 9)

NT = ((1,), (1,))
NN = ((1,), (0,))
TN = ((0,), (0,))


def dot(a, b, dims):
    return lax.dot_general(a, b, (dims, ((), ())), preferred_element_type=F32)


def span(i, size):
    return pl.ds(i * size if isinstance(i, int) else pl.multiple_of(i * size, size), size)


def layer_kernel(
    n,
    residual, qw, kw, vw, dw, gw, qn, kn, vn, dn, gn, gain, outw, outn, mgain, up, down,
    out,
    q_all, k_all, d_all, v_wide, v_narrow, g_wide, g_narrow, w_out, res, d_shard, weights,
    within_all, keys_all, snaps, offsets, total, state, local_w, local_n, carried,
    e1s, e1r, chain_s, chain_r, e2s, prefix,
    gated, partial, near_r, pair_s, cross_r, stream, normed, hidden,
    r1, mix, r2,
    load, ring_s, ring_v, e1_s, e1_v, ch_s, ch_v, e2_s, e2_v,
    na_s, na_v, cr_s, cr_v, st_s, st_v, s1, v1, s2, v2,
):
    s, t = lax.axis_index("sp"), lax.axis_index("tp")
    z, y = s // 2, lax.rem(s, 2)
    m, half_ring = n // 2, n // 2
    u = lax.rem(t, 2)
    near, far = t + 1 - 2 * u, lax.rem(t + 2, 4)
    cross = lax.rem(near + 2, 4)
    tokens, wide = qw.shape
    keys = wide + qn.shape[1]
    values = vw.shape[1]
    groups = ((0, wide, v_wide, local_w), (wide, keys, v_narrow, local_n))

    rows_chunk = tokens // ROW_CHUNKS
    half_rows = rows_chunk // 2
    shard_rows = up.shape[0]
    pairs = [
        (up, weights.at[0, span(s, shard_rows)]),
        (dw, d_all.at[:, :wide]), (dn, d_all.at[:, wide:]),
        (kw, k_all.at[:, :wide]), (kn, k_all.at[:, wide:]),
        (vw, v_wide), (vn, v_narrow),
        (down, d_shard),
        (qw, q_all.at[:, :wide]), (qn, q_all.at[:, wide:]),
        (gw, g_wide), (gn, g_narrow),
        (outw, w_out.at[:values]), (outn, w_out.at[values:]),
    ] + [
        (residual.at[pl.ds(pl.multiple_of(c * rows_chunk + u * half_rows, half_rows), half_rows)],
         res.at[c])
        for c in range(ROW_CHUNKS)
    ]
    loads = [
        pltpu.make_async_copy(a, b, load.at[i]) for i, (a, b) in enumerate(pairs)
    ]
    for copy in loads:
        copy.start()

    total[...] = jnp.zeros_like(total)
    state[...] = jnp.zeros_like(state)

    place = jnp.where(y == 0, z, n - 1 - z)

    def index_of(p):
        p = lax.rem(p + 2 * n, n)
        return jnp.where(p < m, 2 * p, 2 * (n - 1 - p) + 1)

    barrier = pltpu.get_barrier_semaphore()
    partner = s + 1 - 2 * y
    for other in (index_of(place + 1), index_of(place - 1), partner):
        pl.semaphore_signal(barrier, inc=1, device_id={"sp": other}, device_id_type=MESH)
    for other in (near, far):
        pl.semaphore_signal(barrier, inc=1, device_id={"tp": other}, device_id_type=MESH)
    pl.semaphore_wait(barrier, 5)

    cut = shard_rows // 2

    def hop_copy(kind, dist, first, side):
        way = lax.rem(side + y, 2)
        step = 1 - 2 * way
        piece = way if first else 1 - way
        origin = index_of(place - step * (dist - 1))
        rows = pl.ds(pl.multiple_of(origin * shard_rows + piece * cut, cut), cut)
        return pltpu.make_async_remote_copy(
            src_ref=weights.at[kind, rows], dst_ref=weights.at[kind, rows],
            send_sem=ring_s.at[kind, way, dist - 1, piece],
            recv_sem=ring_v.at[kind, way, dist - 1, piece],
            device_id={"sp": index_of(place + step)}, device_id_type=MESH,
        )

    def hop(kind, dist, first, side):
        if dist > 1:
            hop_copy(kind, dist - 1, first, side).wait_recv()
        hop_copy(kind, dist, first, side).start()

    def hops(kind, dist, sides):
        for first in (True, False) if dist < half_ring else (True,):
            for side in sides:
                hop(kind, dist, first, side)

    def arrive(kind):
        for side in (0, 1):
            hop_copy(kind, half_ring, True, side).wait_recv()
            if half_ring > 1:
                hop_copy(kind, half_ring - 1, False, side).wait_recv()

    loads[0].wait()
    hop(0, 1, True, 0)
    hop(0, 1, True, 1)

    block = min(128, tokens)
    blocks = tokens // block
    tril = lax.broadcasted_iota(jnp.int32, (block, block), 0) >= lax.broadcasted_iota(
        jnp.int32, (block, block), 1
    )
    ones = tril.astype(F32).astype(BF)
    for copy in loads[1:7]:
        copy.wait()

    def pass_one(i, carry):
        rows = span(i, block)
        decay = d_all[rows, :].astype(F32)
        g = (jnp.minimum(decay, 0.0) - jnp.log(1.0 + jnp.exp(-jnp.abs(decay)))) / DECAY_NORMALIZER
        high = g.astype(BF)
        low = (g - high.astype(F32)).astype(BF)
        within = dot(ones, high, NN) + dot(ones, low, NN)
        within_all[rows, :] = within
        mid = within[block // 2 - 1 : block // 2]
        last = within[block - 1 : block]
        scaled = k_all[rows, :].astype(F32) * jnp.exp(mid - within)
        keys_all[rows, :] = scaled.astype(BF)
        ends = (scaled * jnp.exp(last - mid)).astype(BF)
        fade = jnp.exp(last)
        for lo, hi, v, _ in groups:
            before = state[:, lo:hi]
            snaps[i, :, lo:hi] = before.astype(BF)
            state[:, lo:hi] = before * fade[:, lo:hi] + dot(v[rows, :], ends[:, lo:hi], TN)
        offsets[i] = total[...]
        total[...] = total[...] + last
        return carry

    lax.fori_loop(0, blocks, pass_one, 0, unroll=2)

    half = values // 2
    part = half // SCAN_CHUNKS
    mine = jnp.exp(total[...])
    mine_high = mine.astype(BF)
    mine_low = (mine - mine_high.astype(F32)).astype(BF)
    e1s[:8, :] = jnp.broadcast_to(mine_high.astype(F32), (8, keys)).astype(BF)
    e1s[8:16, :] = jnp.broadcast_to(mine_low.astype(F32), (8, keys)).astype(BF)
    e1s[16:, :] = state[span(1 - y, half), :].astype(BF)

    def e1_copy(c):
        where = pl.ds(0, 16 + part) if c == 0 else pl.ds(16 + c * part, part)
        return pltpu.make_async_remote_copy(
            src_ref=e1s.at[where], dst_ref=e1r.at[where], send_sem=e1_s.at[c],
            recv_sem=e1_v.at[c], device_id={"sp": partner}, device_id_type=MESH,
        )

    def chain_copy(c):
        where = pl.ds(c * part, part)
        return pltpu.make_async_remote_copy(
            src_ref=chain_s.at[where], dst_ref=chain_r.at[where], send_sem=ch_s.at[c],
            recv_sem=ch_v.at[c], device_id={"sp": lax.rem(s + 2, n)}, device_id_type=MESH,
        )

    def e2_copy(c):
        return pltpu.make_async_remote_copy(
            src_ref=e2s.at[pl.ds(c * part, part)],
            dst_ref=prefix.at[pl.ds(pl.multiple_of(y * half + c * part, part), part)],
            send_sem=e2_s.at[c], recv_sem=e2_v.at[c], device_id={"sp": partner},
            device_id_type=MESH,
        )

    for c in range(SCAN_CHUNKS):
        e1_copy(c).start()

    hop(0, 1, False, 1)
    hop(0, 1, False, 0)
    loads[7].wait()
    weights[1, span(s, shard_rows), :] = d_shard[...].T
    inner_pair = z > 0
    early_a = z >= 2

    @pl.when(inner_pair)
    def _():
        hop(1, 1, True, 1)
        hop(1, 1, False, 1)

    @pl.when(early_a)
    def _():
        hop(1, 1, True, 0)

    for copy in loads[8:10]:
        copy.wait()
    column = lax.broadcasted_iota(jnp.int32, (1, keys), 1)
    scale = jnp.where(column < wide, wide ** -0.5, (keys - wide) ** -0.5).astype(F32)

    def pass_two(i, carry):
        rows = span(i, block)
        within = within_all[rows, :]
        mid = within[block // 2 - 1 : block // 2]
        scaled = q_all[rows, :].astype(F32) * scale * jnp.exp(within - mid)
        whole = scaled * jnp.exp(mid)
        scaled = scaled.astype(BF)
        carried[rows, :] = (whole * jnp.exp(offsets[i])).astype(BF)
        whole = whole.astype(BF)
        for lo, hi, v, local in groups:
            scores = dot(scaled[:, lo:hi], keys_all[rows, lo:hi], NT)
            scores = jnp.where(tril, scores, 0.0).astype(BF)
            local[rows, :] = (
                dot(scores, v[rows, :], NN) + dot(whole[:, lo:hi], snaps[i, :, lo:hi], NT)
            ).astype(BF)
        return carry

    ahead = jnp.minimum(z * (blocks // 2), blocks)
    lax.fori_loop(0, ahead, pass_two, 0)

    @pl.when(z == 0)
    def _():
        chain_r[...] = jnp.zeros_like(chain_r)

    for c in range(SCAN_CHUNKS):
        e1_copy(c).wait_recv()

        @pl.when(z > 0)
        def _():
            chain_copy(c).wait_recv()

        other = e1r[:8, :].astype(F32)[:1] + e1r[8:16, :].astype(F32)[:1]
        fade_even = jnp.where(y == 0, mine, other)
        fade_odd = jnp.where(y == 0, other, mine)
        where = pl.ds(c * part, part)
        own = state[pl.ds(pl.multiple_of(y * half + c * part, part), part), :]
        theirs = e1r[16 + c * part : 16 + (c + 1) * part, :].astype(F32)
        even = jnp.where(y == 0, own, theirs)
        odd = jnp.where(y == 0, theirs, own)
        before = chain_r[where, :].astype(F32)
        between = before * fade_even + even
        chain_s[where, :] = (between * fade_odd + odd).astype(BF)

        @pl.when(z < m - 1)
        def _():
            chain_copy(c).start()

        prefix[pl.ds(pl.multiple_of(y * half + c * part, part), part), :] = jnp.where(
            y == 0, before, between
        ).astype(BF)
        e2s[where, :] = jnp.where(y == 0, between, before).astype(BF)
        e2_copy(c).start()

    @pl.when(jnp.logical_not(inner_pair))
    def _():
        hop(1, 1, True, 1)
        hop(1, 1, False, 1)

    def up_side():
        if half_ring >= 2:
            hops(0, 2, (0,))

        @pl.when(jnp.logical_not(early_a))
        def _():
            hop(1, 1, True, 0)

        hop(1, 1, False, 0)

    pl.when(z < m - 1)(up_side)
    if half_ring >= 2:
        hops(0, 2, (1,))

    lax.fori_loop(ahead, blocks, pass_two, 0)
    for copy in loads[10:]:
        copy.wait()
    for c in range(SCAN_CHUNKS):
        e2_copy(c).wait_recv()
    pl.when(z == m - 1)(up_side)

    def near_copy(c):
        return pltpu.make_async_remote_copy(
            src_ref=partial.at[
                pl.ds(pl.multiple_of(c * rows_chunk + (1 - u) * half_rows, half_rows), half_rows)
            ],
            dst_ref=near_r.at[c], send_sem=na_s.at[c], recv_sem=na_v.at[c],
            device_id={"tp": near}, device_id_type=MESH,
        )

    def cross_copy(c):
        return pltpu.make_async_remote_copy(
            src_ref=pair_s.at[c], dst_ref=cross_r.at[c], send_sem=cr_s.at[c],
            recv_sem=cr_v.at[c], device_id={"tp": far}, device_id_type=MESH,
        )

    def own_rows(c):
        return pl.ds(pl.multiple_of(c * rows_chunk + u * half_rows, half_rows), half_rows)

    def other_rows(c):
        return pl.ds(
            pl.multiple_of(c * rows_chunk + (1 - u) * half_rows, half_rows), half_rows
        )

    def stream_copy(c):
        return pltpu.make_async_remote_copy(
            src_ref=stream.at[own_rows(c)], dst_ref=stream.at[own_rows(c)],
            send_sem=st_s.at[c], recv_sem=st_v.at[c],
            device_id={"tp": near}, device_id_type=MESH,
        )

    width = w_out.shape[1]
    tile = min(512, width)

    def project(c, carry):
        rows = span(c, rows_chunk)
        for j, (lo, hi, _, local) in enumerate(groups):
            gate = (g_wide, g_narrow)[j]
            x = local[rows, :].astype(F32) + dot(carried[rows, lo:hi], prefix[:, lo:hi], NT)
            fit = lax.rsqrt(jnp.mean(jnp.square(x), axis=-1, keepdims=True) + EPS)
            v = gate[rows, :].astype(F32)
            gated[:, j * values : (j + 1) * values] = (
                x * fit * gain[...] * (v / (1.0 + jnp.exp(-v)))
            ).astype(BF)
        for lo in range(0, width, tile):
            partial[rows, lo : lo + tile] = dot(
                gated[...], w_out[:, lo : lo + tile], NN
            ).astype(BF)
        near_copy(c).start()

        @pl.when(c > 0)
        def _():
            pair(c - 1)

        return carry

    def pair(c):
        near_copy(c).wait_recv()
        pair_s[c] = (partial[own_rows(c), :].astype(F32) + near_r[c].astype(F32)).astype(BF)
        cross_copy(c).start()

    lax.fori_loop(0, ROW_CHUNKS, project, 0)
    pair(ROW_CHUNKS - 1)

    def norm(rows):
        x = stream[rows, :].astype(F32)
        fit = lax.rsqrt(jnp.mean(jnp.square(x), axis=1, keepdims=True) + EPS)
        normed[rows, :] = (x * fit * mgain[...]).astype(BF)

    def settle(c):
        cross_copy(c).wait_recv()
        value = pair_s[c].astype(F32) + cross_r[c].astype(F32)
        stream[own_rows(c), :] = (res[c].astype(F32) + value).astype(BF)
        stream_copy(c).start()
        norm(own_rows(c))
        stream_copy(c).wait_recv()
        norm(other_rows(c))

    inner = up.shape[1]
    tile_h = min(512, inner)

    def expand(c, carry):
        expand_rows(span(c, tokens // EXPAND_CHUNKS))
        return carry

    def expand_rows(rows):
        for lo in range(0, inner, tile_h):
            h = dot(normed[rows, :], weights[0, :, lo : lo + tile_h], NN)
            hidden[rows, lo : lo + tile_h] = jnp.square(jnp.maximum(h, 0.0)).astype(BF)

    later = []
    for dist in range(2, half_ring + 1):
        later += [(0, dist + 1, True), (0, dist + 1, False), (1, dist, True), (1, dist, False)]
    later = [h for h in later if h[1] < half_ring or (h[1] == half_ring and h[2])]
    points = POINTS
    each = -(-len(later) // 6)
    due = [points[i] if half_ring == 4 else i // each for i in range(len(later))]

    def serve(point):
        for (kind, dist, is_first), at in zip(later, due):
            if at == point:
                for side in (1, 0):
                    hop(kind, dist, is_first, side)

    own_width = out.shape[1]
    by_shard = shard_rows % 256 == 0 and half_ring >= 3
    shard = max(shard_rows, 128)
    shards = width // shard
    per = own_width // shard
    pieces = 2 if by_shard else 1
    lanes = shard // pieces
    row_parts = (pl.ds(0, tokens - rows_chunk), pl.ds(tokens - rows_chunk, rows_chunk))

    def at_lane(i):
        return pl.ds(i if isinstance(i, int) else pl.multiple_of(i, lanes), lanes)

    def to_near(which, q, j, h, piece):
        return pltpu.make_async_remote_copy(
            src_ref=partial.at[row_parts[h], at_lane(j * shard + piece * lanes)],
            dst_ref=r1.at[which, q, row_parts[h], at_lane(piece * lanes)],
            send_sem=s1.at[which, q, h, piece], recv_sem=v1.at[which, q, h, piece],
            device_id={"tp": near}, device_id_type=MESH,
        )

    def to_far(q, h, piece):
        where = (q, row_parts[h], at_lane(piece * lanes))
        return pltpu.make_async_remote_copy(
            src_ref=mix.at[where], dst_ref=r2.at[where],
            send_sem=s2.at[q, h, piece], recv_sem=v2.at[q, h, piece],
            device_id={"tp": far}, device_id_type=MESH,
        )

    def place_of(k):
        if by_shard:
            dist = (k + 1) // 2
            k = index_of(place + jnp.where(lax.rem(k, 2) == 1, dist, -dist))
        return k, lax.rem(k, per), k // per

    def pieces_of(k, part):
        if part is None:
            return list(range(pieces))
        return [lax.rem(k, 2) if part == 0 else 1 - lax.rem(k, 2)]

    def across(k, h, part):
        j, q, owner = place_of(k)

        @pl.when(owner == far)
        def _():
            for piece in pieces_of(k, part):
                to_near(1, q, j, h, piece).wait_recv()
                here = (q, row_parts[h], at_lane(piece * lanes))
                mine = partial[row_parts[h], at_lane(j * shard + piece * lanes)]
                mix[here] = (mine.astype(F32) + r1[(1,) + here].astype(F32)).astype(BF)
                to_far(q, h, piece).start()

    def contract(k, h, part):
        j, q, owner = place_of(k)
        which = pieces_of(k, part)
        size = shard if part is None else lanes
        start = pl.multiple_of(j * shard + (0 if part is None else which[0] * lanes), lanes)
        columns = pl.ds(start, size)
        partial[row_parts[h], columns] = dot(
            hidden[row_parts[h], :], weights[1, columns, :], NT
        ).astype(BF)

        @pl.when(owner == near)
        def _():
            for piece in which:
                to_near(0, q, j, h, piece).start()

        @pl.when(owner == cross)
        def _():
            for piece in which:
                to_near(1, q, j, h, piece).start()

    pending = []

    def flush():
        while pending:
            across(*pending.pop())

    def run(order, h, part=None):
        def look(i):
            value = order[0]
            for n_row, k in enumerate(order[1:], 1):
                value = jnp.where(i == n_row, k, value)
            return value

        def step(i, carry):
            contract(look(i), h, part)
            if pending:
                pl.when(i == 0)(lambda: across(*pending[0]))
            pl.when(i > 0)(lambda: across(look(i - 1), h, part))
            return carry

        lax.fori_loop(0, len(order), step, 0)
        pending[:] = [(jnp.int32(order[-1]), h, part)]

    near_by = 2 * (half_ring - 2) + 1
    close_order = [near_by - 1, near_by - 2] + list(range(near_by - 2))
    third = [near_by, near_by + 1]

    serve(0)
    per_expand = ROW_CHUNKS // EXPAND_CHUNKS
    for c in range(ROW_CHUNKS):
        settle(c)
        serve(c + 1)
        if c == ROW_CHUNKS - per_expand - 1:
            arrive(0)
            lax.fori_loop(0, EXPAND_CHUNKS - 1, expand, 0)
            for i in range(ROW_CHUNKS):
                near_copy(i).wait_send()
        if c >= ROW_CHUNKS - per_expand:
            expand_rows(span(c, rows_chunk))
        if c == ROW_CHUNKS - 2 and by_shard:
            run(close_order, 0)
            serve(ROW_CHUNKS + 1)
            run(third, 0, 0)
            flush()
    if by_shard:
        run(close_order, 1)
        run(third, 1, 0)
        for side in (0, 1):
            hop_copy(1, half_ring - 1, False, side).wait_recv()
        run(third, 0, 1)
        run(third, 1, 1)
        for side in (0, 1):
            hop_copy(1, half_ring, True, side).wait_recv()
        run([shards - 1], 0)
        run([shards - 1], 1)
    else:
        arrive(1)
        for h in (0, 1):
            run(list(range(shards)), h)
    flush()

    for c in range(SCAN_CHUNKS):
        e1_copy(c).wait_send()
        e2_copy(c).wait_send()

        @pl.when(z < m - 1)
        def _():
            chain_copy(c).wait_send()

    for c in range(ROW_CHUNKS):
        cross_copy(c).wait_send()
        stream_copy(c).wait_send()
    for kind in (0, 1):
        for dist in range(1, half_ring + 1):
            for is_first in (True, False) if dist < half_ring else (True,):
                for side in (0, 1):
                    hop_copy(kind, dist, is_first, side).wait_send()

    for q in range(per):
        for h in (0, 1):
            for piece in range(pieces):
                to_near(0, q, near * per + q, h, piece).wait_send()
                to_near(1, q, cross * per + q, h, piece).wait_send()

    for h in (0, 1):
        for q in range(per):
            for piece in range(pieces):
                j = t * per + q
                rows = row_parts[h]
                to_near(0, q, j, h, piece).wait_recv()
                to_far(q, h, piece).wait_recv()
                columns = at_lane(j * shard + piece * lanes)
                inside = at_lane(piece * lanes)
                value = partial[rows, columns].astype(F32) + r1[0, q, rows, inside].astype(F32)
                value = value + r2[q, rows, inside].astype(F32)
                lo = q * shard + piece * lanes
                out[rows, lo : lo + lanes] = (
                    stream[rows, columns].astype(F32) + value
                ).astype(BF)
    for q in range(per):
        for h in (0, 1):
            for piece in range(pieces):
                to_far(q, h, piece).wait_send()


def layer(n, *args):
    (residual, qw, kw, vw, dw, gw, qn, kn, vn, dn, gn, gain, outw, outn, mgain, up, down) = args
    tokens, wide = qw.shape
    keys = wide + qn.shape[1]
    values = vw.shape[1]
    width = outw.shape[1]
    inner = up.shape[1]
    own_width = width // 4
    block = min(128, tokens)
    blocks = tokens // block
    rc = tokens // ROW_CHUNKS
    hr = rc // 2
    anyspace = pl.BlockSpec(memory_space=pl.ANY)
    vspace = pl.BlockSpec(memory_space=VM)
    half = values // 2
    shard = max(down.shape[1], 128)
    per = own_width // shard
    scratch = [
        VM((tokens, keys), BF), VM((tokens, keys), BF), VM((tokens, keys), BF),
        VM((tokens, values), BF), VM((tokens, values), BF),
        VM((tokens, values), BF), VM((tokens, values), BF),
        VM((2 * values, width), BF), VM((ROW_CHUNKS, hr, width), BF),
        VM(down.shape, BF), VM((2, n * up.shape[0], inner), BF),
        VM((tokens, keys), F32), VM((tokens, keys), BF), VM((blocks, values, keys), BF),
        VM((blocks, 1, keys), F32), VM((1, keys), F32), VM((values, keys), F32),
        VM((tokens, values), BF), VM((tokens, values), BF), VM((tokens, keys), BF),
        VM((16 + half, keys), BF), VM((16 + half, keys), BF),
        VM((half, keys), BF), VM((half, keys), BF), VM((half, keys), BF),
        VM((values, keys), BF),
        VM((rc, 2 * values), BF), VM((tokens, width), BF),
        VM((ROW_CHUNKS, hr, width), BF), VM((ROW_CHUNKS, hr, width), BF),
        VM((ROW_CHUNKS, hr, width), BF),
        VM((tokens, width), BF), VM((tokens, width), BF), VM((tokens, inner), BF),
        VM((2, per, tokens, shard), BF), VM((per, tokens, shard), BF),
        VM((per, tokens, shard), BF),
        DMA((14 + ROW_CHUNKS,)),
        DMA((2, 2, n // 2, 2)), DMA((2, 2, n // 2, 2)),
    ] + [DMA((SCAN_CHUNKS,))] * 6 + [DMA((ROW_CHUNKS,))] * 6 + [
        DMA((2, per, 2, 2)), DMA((2, per, 2, 2)), DMA((per, 2, 2)), DMA((per, 2, 2)),
    ]
    in_specs = [anyspace] * 17
    in_specs[11] = in_specs[14] = vspace
    return pl.pallas_call(
        functools.partial(layer_kernel, n),
        out_shape=VM((tokens, own_width), BF),
        in_specs=in_specs,
        out_specs=vspace,
        scratch_shapes=scratch,
        compiler_params=pltpu.CompilerParams(
            collective_id=0, has_side_effects=True, vmem_limit_bytes=60 * 2**20
        ),
        cost_estimate=pl.CostEstimate(
            flops=30 * 10**9, bytes_accessed=32 * 2**20, transcendentals=0
        ),
        name="layer",
    )(*args)


def body(*args):
    n_sp, n_tp = lax.axis_size("sp"), lax.axis_size("tp")
    assert n_tp == HEADS == 4 and n_sp % 2 == 0
    args = list(args)
    args[11] = args[11].reshape(1, -1)
    args[14] = args[14].reshape(1, -1)
    return layer(n_sp, *args)


def solution(mesh):
    return jax.shard_map(
        body,
        mesh=mesh,
        in_specs=(
            P("sp", None),
            P("sp", "tp"),
            P("sp", "tp"),
            P("sp", "tp"),
            P("sp", "tp"),
            P("sp", "tp"),
            P("sp", "tp"),
            P("sp", "tp"),
            P("sp", "tp"),
            P("sp", "tp"),
            P("sp", "tp"),
            P(),
            P("tp", None),
            P("tp", None),
            P(),
            P("sp", "tp"),
            P("tp", "sp"),
        ),
        out_specs=P("sp", "tp"),
        check_vma=False,
    )
```

```python
import functools
import jax
import jax.numpy as jnp
from jax import lax
from jax.experimental import pallas as pl
from jax.experimental.pallas import tpu as pltpu
from jax.sharding import PartitionSpec as P

HEADS = 4
EPS = 1e-05
DECAY_NORMALIZER = 16.0
MESH = pl.DeviceIdType.MESH
BF = jnp.bfloat16
F32 = jnp.float32
VM = pltpu.VMEM
DMA = pltpu.SemaphoreType.DMA
SCAN_CHUNKS = 8
ROW_CHUNKS = 8
EXPAND_CHUNKS = 4
POINTS = (0, 0, 3, 4, 2, 6, 7, 9)

NT = ((1,), (1,))
NN = ((1,), (0,))
TN = ((0,), (0,))


def dot(a, b, dims):
    return lax.dot_general(a, b, (dims, ((), ())), preferred_element_type=F32)


def span(i, size):
    return pl.ds(i * size if isinstance(i, int) else pl.multiple_of(i * size, size), size)


def layer_kernel(
    n,
    residual, qw, kw, vw, dw, gw, qn, kn, vn, dn, gn, gain, outw, outn, mgain, up, down,
    out,
    q_all, k_all, d_all, v_wide, v_narrow, g_wide, g_narrow, w_out, res, d_shard, weights,
    within_all, keys_all, snaps, offsets, total, state, local_w, local_n, carried,
    e1s, e1r, chain_s, chain_r, e2s, prefix,
    gated, partial, near_r, pair_s, cross_r, stream, normed, hidden,
    r1, mix, r2,
    load, ring_s, ring_v, e1_s, e1_v, ch_s, ch_v, e2_s, e2_v,
    na_s, na_v, cr_s, cr_v, st_s, st_v, s1, v1, s2, v2,
):
    s, t = lax.axis_index("sp"), lax.axis_index("tp")
    z, y = s // 2, lax.rem(s, 2)
    m, half_ring = n // 2, n // 2
    u = lax.rem(t, 2)
    near, far = t + 1 - 2 * u, lax.rem(t + 2, 4)
    cross = lax.rem(near + 2, 4)
    tokens, wide = qw.shape
    keys = wide + qn.shape[1]
    values = vw.shape[1]
    groups = ((0, wide, v_wide, local_w), (wide, keys, v_narrow, local_n))

    rows_chunk = tokens // ROW_CHUNKS
    half_rows = rows_chunk // 2
    shard_rows = up.shape[0]
    pairs = [
        (up, weights.at[0, span(s, shard_rows)]),
        (dw, d_all.at[:, :wide]), (dn, d_all.at[:, wide:]),
        (kw, k_all.at[:, :wide]), (kn, k_all.at[:, wide:]),
        (vw, v_wide), (vn, v_narrow),
        (down, d_shard),
        (qw, q_all.at[:, :wide]), (qn, q_all.at[:, wide:]),
        (gw, g_wide), (gn, g_narrow),
        (outw, w_out.at[:values]), (outn, w_out.at[values:]),
    ] + [
        (residual.at[pl.ds(pl.multiple_of(c * rows_chunk + u * half_rows, half_rows), half_rows)],
         res.at[c])
        for c in range(ROW_CHUNKS)
    ]
    loads = [
        pltpu.make_async_copy(a, b, load.at[i]) for i, (a, b) in enumerate(pairs)
    ]
    for copy in loads:
        copy.start()

    total[...] = jnp.zeros_like(total)
    state[...] = jnp.zeros_like(state)

    place = jnp.where(y == 0, z, n - 1 - z)

    def index_of(p):
        p = lax.rem(p + 2 * n, n)
        return jnp.where(p < m, 2 * p, 2 * (n - 1 - p) + 1)

    barrier = pltpu.get_barrier_semaphore()
    partner = s + 1 - 2 * y
    for other in (index_of(place + 1), index_of(place - 1), partner):
        pl.semaphore_signal(barrier, inc=1, device_id={"sp": other}, device_id_type=MESH)
    for other in (near, far):
        pl.semaphore_signal(barrier, inc=1, device_id={"tp": other}, device_id_type=MESH)
    pl.semaphore_wait(barrier, 5)

    cut = shard_rows // 2

    def hop_copy(kind, dist, first, side):
        way = lax.rem(side + y, 2)
        step = 1 - 2 * way
        piece = way if first else 1 - way
        origin = index_of(place - step * (dist - 1))
        rows = pl.ds(pl.multiple_of(origin * shard_rows + piece * cut, cut), cut)
        return pltpu.make_async_remote_copy(
            src_ref=weights.at[kind, rows], dst_ref=weights.at[kind, rows],
            send_sem=ring_s.at[kind, way, dist - 1, piece],
            recv_sem=ring_v.at[kind, way, dist - 1, piece],
            device_id={"sp": index_of(place + step)}, device_id_type=MESH,
        )

    def hop(kind, dist, first, side):
        if dist > 1:
            hop_copy(kind, dist - 1, first, side).wait_recv()
        hop_copy(kind, dist, first, side).start()

    def hops(kind, dist, sides):
        for first in (True, False) if dist < half_ring else (True,):
            for side in sides:
                hop(kind, dist, first, side)

    def arrive(kind):
        for side in (0, 1):
            hop_copy(kind, half_ring, True, side).wait_recv()
            if half_ring > 1:
                hop_copy(kind, half_ring - 1, False, side).wait_recv()

    loads[0].wait()
    hop(0, 1, True, 0)
    hop(0, 1, True, 1)

    block = min(128, tokens)
    blocks = tokens // block
    tril = lax.broadcasted_iota(jnp.int32, (block, block), 0) >= lax.broadcasted_iota(
        jnp.int32, (block, block), 1
    )
    ones = tril.astype(F32).astype(BF)
    for copy in loads[1:7]:
        copy.wait()

    def pass_one(i, carry):
        rows = span(i, block)
        decay = d_all[rows, :].astype(F32)
        g = (jnp.minimum(decay, 0.0) - jnp.log(1.0 + jnp.exp(-jnp.abs(decay)))) / DECAY_NORMALIZER
        high = g.astype(BF)
        low = (g - high.astype(F32)).astype(BF)
        within = dot(ones, high, NN) + dot(ones, low, NN)
        within_all[rows, :] = within
        mid = within[block // 2 - 1 : block // 2]
        last = within[block - 1 : block]
        scaled = k_all[rows, :].astype(F32) * jnp.exp(mid - within)
        keys_all[rows, :] = scaled.astype(BF)
        ends = (scaled * jnp.exp(last - mid)).astype(BF)
        fade = jnp.exp(last)
        for lo, hi, v, _ in groups:
            before = state[:, lo:hi]
            snaps[i, :, lo:hi] = before.astype(BF)
            state[:, lo:hi] = before * fade[:, lo:hi] + dot(v[rows, :], ends[:, lo:hi], TN)
        offsets[i] = total[...]
        total[...] = total[...] + last
        return carry

    lax.fori_loop(0, blocks, pass_one, 0, unroll=2)

    half = values // 2
    part = half // SCAN_CHUNKS
    mine = jnp.exp(total[...])
    mine_high = mine.astype(BF)
    mine_low = (mine - mine_high.astype(F32)).astype(BF)
    e1s[:8, :] = jnp.broadcast_to(mine_high.astype(F32), (8, keys)).astype(BF)
    e1s[8:16, :] = jnp.broadcast_to(mine_low.astype(F32), (8, keys)).astype(BF)
    e1s[16:, :] = state[span(1 - y, half), :].astype(BF)

    def e1_copy(c):
        where = pl.ds(0, 16 + part) if c == 0 else pl.ds(16 + c * part, part)
        return pltpu.make_async_remote_copy(
            src_ref=e1s.at[where], dst_ref=e1r.at[where], send_sem=e1_s.at[c],
            recv_sem=e1_v.at[c], device_id={"sp": partner}, device_id_type=MESH,
        )

    def chain_copy(c):
        where = pl.ds(c * part, part)
        return pltpu.make_async_remote_copy(
            src_ref=chain_s.at[where], dst_ref=chain_r.at[where], send_sem=ch_s.at[c],
            recv_sem=ch_v.at[c], device_id={"sp": lax.rem(s + 2, n)}, device_id_type=MESH,
        )

    def e2_copy(c):
        return pltpu.make_async_remote_copy(
            src_ref=e2s.at[pl.ds(c * part, part)],
            dst_ref=prefix.at[pl.ds(pl.multiple_of(y * half + c * part, part), part)],
            send_sem=e2_s.at[c], recv_sem=e2_v.at[c], device_id={"sp": partner},
            device_id_type=MESH,
        )

    for c in range(SCAN_CHUNKS):
        e1_copy(c).start()

    hop(0, 1, False, 1)
    hop(0, 1, False, 0)
    loads[7].wait()
    weights[1, span(s, shard_rows), :] = d_shard[...].T
    inner_pair = z > 0
    early_a = z >= 2

    @pl.when(inner_pair)
    def _():
        hop(1, 1, True, 1)
        hop(1, 1, False, 1)

    @pl.when(early_a)
    def _():
        hop(1, 1, True, 0)

    for copy in loads[8:10]:
        copy.wait()
    column = lax.broadcasted_iota(jnp.int32, (1, keys), 1)
    scale = jnp.where(column < wide, wide ** -0.5, (keys - wide) ** -0.5).astype(F32)

    def pass_two(i, carry):
        rows = span(i, block)
        within = within_all[rows, :]
        mid = within[block // 2 - 1 : block // 2]
        scaled = q_all[rows, :].astype(F32) * scale * jnp.exp(within - mid)
        whole = scaled * jnp.exp(mid)
        scaled = scaled.astype(BF)
        carried[rows, :] = (whole * jnp.exp(offsets[i])).astype(BF)
        whole = whole.astype(BF)
        for lo, hi, v, local in groups:
            scores = dot(scaled[:, lo:hi], keys_all[rows, lo:hi], NT)
            scores = jnp.where(tril, scores, 0.0).astype(BF)
            local[rows, :] = (
                dot(scores, v[rows, :], NN) + dot(whole[:, lo:hi], snaps[i, :, lo:hi], NT)
            ).astype(BF)
        return carry

    ahead = jnp.minimum(z * (blocks // 2), blocks)
    lax.fori_loop(0, ahead, pass_two, 0)

    @pl.when(z == 0)
    def _():
        chain_r[...] = jnp.zeros_like(chain_r)

    for c in range(SCAN_CHUNKS):
        e1_copy(c).wait_recv()

        @pl.when(z > 0)
        def _():
            chain_copy(c).wait_recv()

        other = e1r[:8, :].astype(F32)[:1] + e1r[8:16, :].astype(F32)[:1]
        fade_even = jnp.where(y == 0, mine, other)
        fade_odd = jnp.where(y == 0, other, mine)
        where = pl.ds(c * part, part)
        own = state[pl.ds(pl.multiple_of(y * half + c * part, part), part), :]
        theirs = e1r[16 + c * part : 16 + (c + 1) * part, :].astype(F32)
        even = jnp.where(y == 0, own, theirs)
        odd = jnp.where(y == 0, theirs, own)
        before = chain_r[where, :].astype(F32)
        between = before * fade_even + even
        chain_s[where, :] = (between * fade_odd + odd).astype(BF)

        @pl.when(z < m - 1)
        def _():
            chain_copy(c).start()

        prefix[pl.ds(pl.multiple_of(y * half + c * part, part), part), :] = jnp.where(
            y == 0, before, between
        ).astype(BF)
        e2s[where, :] = jnp.where(y == 0, between, before).astype(BF)
        e2_copy(c).start()

    @pl.when(jnp.logical_not(inner_pair))
    def _():
        hop(1, 1, True, 1)
        hop(1, 1, False, 1)

    def up_side():
        if half_ring >= 2:
            hops(0, 2, (0,))

        @pl.when(jnp.logical_not(early_a))
        def _():
            hop(1, 1, True, 0)

        hop(1, 1, False, 0)

    pl.when(z < m - 1)(up_side)
    if half_ring >= 2:
        hops(0, 2, (1,))

    lax.fori_loop(ahead, blocks, pass_two, 0)
    for copy in loads[10:]:
        copy.wait()
    for c in range(SCAN_CHUNKS):
        if c == SCAN_CHUNKS // 2 + 1:
            pl.when(z == m - 1)(up_side)
        e2_copy(c).wait_recv()

    def near_copy(c):
        return pltpu.make_async_remote_copy(
            src_ref=partial.at[
                pl.ds(pl.multiple_of(c * rows_chunk + (1 - u) * half_rows, half_rows), half_rows)
            ],
            dst_ref=near_r.at[c], send_sem=na_s.at[c], recv_sem=na_v.at[c],
            device_id={"tp": near}, device_id_type=MESH,
        )

    def cross_copy(c):
        return pltpu.make_async_remote_copy(
            src_ref=pair_s.at[c], dst_ref=cross_r.at[c], send_sem=cr_s.at[c],
            recv_sem=cr_v.at[c], device_id={"tp": far}, device_id_type=MESH,
        )

    def own_rows(c):
        return pl.ds(pl.multiple_of(c * rows_chunk + u * half_rows, half_rows), half_rows)

    def other_rows(c):
        return pl.ds(
            pl.multiple_of(c * rows_chunk + (1 - u) * half_rows, half_rows), half_rows
        )

    def stream_copy(c):
        return pltpu.make_async_remote_copy(
            src_ref=stream.at[own_rows(c)], dst_ref=stream.at[own_rows(c)],
            send_sem=st_s.at[c], recv_sem=st_v.at[c],
            device_id={"tp": near}, device_id_type=MESH,
        )

    width = w_out.shape[1]
    tile = min(512, width)

    def project(c, carry):
        rows = span(c, rows_chunk)
        for j, (lo, hi, _, local) in enumerate(groups):
            gate = (g_wide, g_narrow)[j]
            x = local[rows, :].astype(F32) + dot(carried[rows, lo:hi], prefix[:, lo:hi], NT)
            fit = lax.rsqrt(jnp.mean(jnp.square(x), axis=-1, keepdims=True) + EPS)
            v = gate[rows, :].astype(F32)
            gated[:, j * values : (j + 1) * values] = (
                x * fit * gain[...] * (v / (1.0 + jnp.exp(-v)))
            ).astype(BF)
        for lo in range(0, width, tile):
            partial[rows, lo : lo + tile] = dot(
                gated[...], w_out[:, lo : lo + tile], NN
            ).astype(BF)
        near_copy(c).start()

        @pl.when(c > 0)
        def _():
            pair(c - 1)

        return carry

    def pair(c):
        near_copy(c).wait_recv()
        pair_s[c] = (partial[own_rows(c), :].astype(F32) + near_r[c].astype(F32)).astype(BF)
        cross_copy(c).start()

    lax.fori_loop(0, ROW_CHUNKS, project, 0)
    pair(ROW_CHUNKS - 1)

    def norm(rows):
        x = stream[rows, :].astype(F32)
        fit = lax.rsqrt(jnp.mean(jnp.square(x), axis=1, keepdims=True) + EPS)
        normed[rows, :] = (x * fit * mgain[...]).astype(BF)

    def settle(c):
        cross_copy(c).wait_recv()
        value = pair_s[c].astype(F32) + cross_r[c].astype(F32)
        stream[own_rows(c), :] = (res[c].astype(F32) + value).astype(BF)
        stream_copy(c).start()
        norm(own_rows(c))
        stream_copy(c).wait_recv()
        norm(other_rows(c))

    inner = up.shape[1]
    tile_h = min(512, inner)

    def expand(c, carry):
        expand_rows(span(c, tokens // EXPAND_CHUNKS))
        return carry

    def expand_rows(rows):
        for lo in range(0, inner, tile_h):
            h = dot(normed[rows, :], weights[0, :, lo : lo + tile_h], NN)
            hidden[rows, lo : lo + tile_h] = jnp.square(jnp.maximum(h, 0.0)).astype(BF)

    later = []
    for dist in range(2, half_ring + 1):
        later += [(0, dist + 1, True), (0, dist + 1, False), (1, dist, True), (1, dist, False)]
    later = [h for h in later if h[1] < half_ring or (h[1] == half_ring and h[2])]
    points = POINTS
    each = -(-len(later) // 6)
    due = [points[i] if half_ring == 4 else i // each for i in range(len(later))]

    def serve(point):
        for (kind, dist, is_first), at in zip(later, due):
            if at == point:
                for side in (1, 0):
                    hop(kind, dist, is_first, side)

    own_width = out.shape[1]
    by_shard = shard_rows % 256 == 0 and half_ring >= 3
    shard = max(shard_rows, 128)
    shards = width // shard
    per = own_width // shard
    pieces = 2 if by_shard else 1
    lanes = shard // pieces
    row_parts = (pl.ds(0, tokens - rows_chunk), pl.ds(tokens - rows_chunk, rows_chunk))

    def at_lane(i):
        return pl.ds(i if isinstance(i, int) else pl.multiple_of(i, lanes), lanes)

    def to_near(which, q, j, h, piece):
        return pltpu.make_async_remote_copy(
            src_ref=partial.at[row_parts[h], at_lane(j * shard + piece * lanes)],
            dst_ref=r1.at[which, q, row_parts[h], at_lane(piece * lanes)],
            send_sem=s1.at[which, q, h, piece], recv_sem=v1.at[which, q, h, piece],
            device_id={"tp": near}, device_id_type=MESH,
        )

    def to_far(q, h, piece):
        where = (q, row_parts[h], at_lane(piece * lanes))
        return pltpu.make_async_remote_copy(
            src_ref=mix.at[where], dst_ref=r2.at[where],
            send_sem=s2.at[q, h, piece], recv_sem=v2.at[q, h, piece],
            device_id={"tp": far}, device_id_type=MESH,
        )

    def place_of(k):
        if by_shard:
            dist = (k + 1) // 2
            k = index_of(place + jnp.where(lax.rem(k, 2) == 1, dist, -dist))
        return k, lax.rem(k, per), k // per

    def pieces_of(k, part):
        if part is None:
            return list(range(pieces))
        return [lax.rem(k, 2) if part == 0 else 1 - lax.rem(k, 2)]

    def across(k, h, part):
        j, q, owner = place_of(k)

        @pl.when(owner == far)
        def _():
            for piece in pieces_of(k, part):
                to_near(1, q, j, h, piece).wait_recv()
                here = (q, row_parts[h], at_lane(piece * lanes))
                mine = partial[row_parts[h], at_lane(j * shard + piece * lanes)]
                mix[here] = (mine.astype(F32) + r1[(1,) + here].astype(F32)).astype(BF)
                to_far(q, h, piece).start()

    def contract(k, h, part):
        j, q, owner = place_of(k)
        which = pieces_of(k, part)
        size = shard if part is None else lanes
        start = pl.multiple_of(j * shard + (0 if part is None else which[0] * lanes), lanes)
        columns = pl.ds(start, size)
        partial[row_parts[h], columns] = dot(
            hidden[row_parts[h], :], weights[1, columns, :], NT
        ).astype(BF)

        @pl.when(owner == near)
        def _():
            for piece in which:
                to_near(0, q, j, h, piece).start()

        @pl.when(owner == cross)
        def _():
            for piece in which:
                to_near(1, q, j, h, piece).start()

    pending = []

    def flush():
        while pending:
            across(*pending.pop())

    def run(order, h, part=None):
        def look(i):
            value = order[0]
            for n_row, k in enumerate(order[1:], 1):
                value = jnp.where(i == n_row, k, value)
            return value

        def step(i, carry):
            contract(look(i), h, part)
            if pending:
                pl.when(i == 0)(lambda: across(*pending[0]))
            pl.when(i > 0)(lambda: across(look(i - 1), h, part))
            return carry

        lax.fori_loop(0, len(order), step, 0)
        pending[:] = [(jnp.int32(order[-1]), h, part)]

    near_by = 2 * (half_ring - 2) + 1
    close_order = [near_by - 1, near_by - 2] + list(range(near_by - 2))
    third = [near_by, near_by + 1]

    serve(0)
    per_expand = ROW_CHUNKS // EXPAND_CHUNKS
    for c in range(ROW_CHUNKS):
        settle(c)
        serve(c + 1)
        if c == ROW_CHUNKS - per_expand - 1:
            arrive(0)
            lax.fori_loop(0, EXPAND_CHUNKS - 1, expand, 0)
            for i in range(ROW_CHUNKS):
                near_copy(i).wait_send()
        if c >= ROW_CHUNKS - per_expand:
            expand_rows(span(c, rows_chunk))
        if c == ROW_CHUNKS - 2 and by_shard:
            run(close_order, 0)
            serve(ROW_CHUNKS + 1)
            run(third, 0, 0)
            flush()
    if by_shard:
        run(close_order, 1)
        run(third, 1, 0)
        for side in (0, 1):
            hop_copy(1, half_ring - 1, False, side).wait_recv()
        run(third, 0, 1)
        run(third, 1, 1)
        for side in (0, 1):
            hop_copy(1, half_ring, True, side).wait_recv()
        run([shards - 1], 0)
        run([shards - 1], 1)
    else:
        arrive(1)
        for h in (0, 1):
            run(list(range(shards)), h)
    flush()

    for c in range(SCAN_CHUNKS):
        e1_copy(c).wait_send()
        e2_copy(c).wait_send()

        @pl.when(z < m - 1)
        def _():
            chain_copy(c).wait_send()

    for c in range(ROW_CHUNKS):
        cross_copy(c).wait_send()
        stream_copy(c).wait_send()
    for kind in (0, 1):
        for dist in range(1, half_ring + 1):
            for is_first in (True, False) if dist < half_ring else (True,):
                for side in (0, 1):
                    hop_copy(kind, dist, is_first, side).wait_send()

    for q in range(per):
        for h in (0, 1):
            for piece in range(pieces):
                to_near(0, q, near * per + q, h, piece).wait_send()
                to_near(1, q, cross * per + q, h, piece).wait_send()

    for h in (0, 1):
        for q in range(per):
            for piece in range(pieces):
                j = t * per + q
                rows = row_parts[h]
                to_near(0, q, j, h, piece).wait_recv()
                to_far(q, h, piece).wait_recv()
                columns = at_lane(j * shard + piece * lanes)
                inside = at_lane(piece * lanes)
                value = partial[rows, columns].astype(F32) + r1[0, q, rows, inside].astype(F32)
                value = value + r2[q, rows, inside].astype(F32)
                lo = q * shard + piece * lanes
                out[rows, lo : lo + lanes] = (
                    stream[rows, columns].astype(F32) + value
                ).astype(BF)
    for q in range(per):
        for h in (0, 1):
            for piece in range(pieces):
                to_far(q, h, piece).wait_send()


def layer(n, *args):
    (residual, qw, kw, vw, dw, gw, qn, kn, vn, dn, gn, gain, outw, outn, mgain, up, down) = args
    tokens, wide = qw.shape
    keys = wide + qn.shape[1]
    values = vw.shape[1]
    width = outw.shape[1]
    inner = up.shape[1]
    own_width = width // 4
    block = min(128, tokens)
    blocks = tokens // block
    rc = tokens // ROW_CHUNKS
    hr = rc // 2
    anyspace = pl.BlockSpec(memory_space=pl.ANY)
    vspace = pl.BlockSpec(memory_space=VM)
    half = values // 2
    shard = max(down.shape[1], 128)
    per = own_width // shard
    scratch = [
        VM((tokens, keys), BF), VM((tokens, keys), BF), VM((tokens, keys), BF),
        VM((tokens, values), BF), VM((tokens, values), BF),
        VM((tokens, values), BF), VM((tokens, values), BF),
        VM((2 * values, width), BF), VM((ROW_CHUNKS, hr, width), BF),
        VM(down.shape, BF), VM((2, n * up.shape[0], inner), BF),
        VM((tokens, keys), F32), VM((tokens, keys), BF), VM((blocks, values, keys), BF),
        VM((blocks, 1, keys), F32), VM((1, keys), F32), VM((values, keys), F32),
        VM((tokens, values), BF), VM((tokens, values), BF), VM((tokens, keys), BF),
        VM((16 + half, keys), BF), VM((16 + half, keys), BF),
        VM((half, keys), BF), VM((half, keys), BF), VM((half, keys), BF),
        VM((values, keys), BF),
        VM((rc, 2 * values), BF), VM((tokens, width), BF),
        VM((ROW_CHUNKS, hr, width), BF), VM((ROW_CHUNKS, hr, width), BF),
        VM((ROW_CHUNKS, hr, width), BF),
        VM((tokens, width), BF), VM((tokens, width), BF), VM((tokens, inner), BF),
        VM((2, per, tokens, shard), BF), VM((per, tokens, shard), BF),
        VM((per, tokens, shard), BF),
        DMA((14 + ROW_CHUNKS,)),
        DMA((2, 2, n // 2, 2)), DMA((2, 2, n // 2, 2)),
    ] + [DMA((SCAN_CHUNKS,))] * 6 + [DMA((ROW_CHUNKS,))] * 6 + [
        DMA((2, per, 2, 2)), DMA((2, per, 2, 2)), DMA((per, 2, 2)), DMA((per, 2, 2)),
    ]
    in_specs = [anyspace] * 17
    in_specs[11] = in_specs[14] = vspace
    return pl.pallas_call(
        functools.partial(layer_kernel, n),
        out_shape=VM((tokens, own_width), BF),
        in_specs=in_specs,
        out_specs=vspace,
        scratch_shapes=scratch,
        compiler_params=pltpu.CompilerParams(
            collective_id=0, has_side_effects=True, vmem_limit_bytes=60 * 2**20
        ),
        cost_estimate=pl.CostEstimate(
            flops=30 * 10**9, bytes_accessed=32 * 2**20, transcendentals=0
        ),
        name="layer",
    )(*args)


def body(*args):
    n_sp, n_tp = lax.axis_size("sp"), lax.axis_size("tp")
    assert n_tp == HEADS == 4 and n_sp % 2 == 0
    args = list(args)
    args[11] = args[11].reshape(1, -1)
    args[14] = args[14].reshape(1, -1)
    return layer(n_sp, *args)


def solution(mesh):
    return jax.shard_map(
        body,
        mesh=mesh,
        in_specs=(
            P("sp", None),
            P("sp", "tp"),
            P("sp", "tp"),
            P("sp", "tp"),
            P("sp", "tp"),
            P("sp", "tp"),
            P("sp", "tp"),
            P("sp", "tp"),
            P("sp", "tp"),
            P("sp", "tp"),
            P("sp", "tp"),
            P(),
            P("tp", None),
            P("tp", None),
            P(),
            P("sp", "tp"),
            P("tp", "sp"),
        ),
        out_specs=P("sp", "tp"),
        check_vma=False,
    )
```
